128 devices in a mesh: fs: 16 (over z, x), tp: 8 (over y, core).
Axes of the slice: x: 4, y: 4, z: 4, core: 2. Of those that a mesh axis runs over, the one named last changes fastest.
Arguments:
- tokens: bfloat16 [32, 384, 2048], P('fs', None, 'tp'), may hold values from -20 to 20
- first_gain: float32 [2048], replicated, may hold values from 0.1 to 1.9
- first_gate: bfloat16 [2048, 5120], P('fs', 'tp'), may hold values from -0.125 to 0.125
- first_up: bfloat16 [2048, 5120], P('fs', 'tp'), may hold values from -0.125 to 0.125
- first_down: bfloat16 [5120, 2048], P('tp', 'fs'), may hold values from -0.078125 to 0.078125
- mixer_gain: float32 [2048], replicated, may hold values from 0.1 to 1.9
- conv_input: bfloat16 [2048, 1024], P('fs', 'tp'), may hold values from -0.125 to 0.125
- outer_gate: bfloat16 [2048, 1024], P('fs', 'tp'), may hold values from -0.125 to 0.125
- inner_gate: bfloat16 [2048, 1024], P('fs', 'tp'), may hold values from -0.125 to 0.125
- conv_taps: float32 [3, 1024], P(None, 'tp'), may hold values from -3.5 to 3.5
- mixer_out: bfloat16 [1024, 2048], P('tp', 'fs'), may hold values from -0.1875 to 0.1875
- second_gain: float32 [2048], replicated, may hold values from 0.1 to 1.9
- second_gate: bfloat16 [2048, 5120], P('fs', 'tp'), may hold values from -0.125 to 0.125
- second_up: bfloat16 [2048, 5120], P('fs', 'tp'), may hold values from -0.125 to 0.125
- second_down: bfloat16 [5120, 2048], P('tp', 'fs'), may hold values from -0.078125 to 0.078125
Outputs:
- layer_out: bfloat16 [32, 384, 2048], P('fs', None, 'tp')
The draws below stay inside these ranges and needn't reach their ends.
All inputs are finite; a program needn't handle non-finite values.
Results may differ from the reference program's by a relative error of at most 0.015.
Values may be sent and summed in bfloat16 or wider, within the bound.
A program may use at most 64 MiB of HBM per device.

```python
import jax
import jax.numpy as jnp
from jax import lax

D = 2048
FF = 5120
CW = 1024
KERNEL = 3
LEN = 384
SEQS = 32
N_TP = 8


def draw_tokens(key, part):
    key_base, key_block, key_scale = jax.random.split(key, 3)
    blocks = jax.random.uniform(key_block, (SEQS, LEN, N_TP, 1), jnp.float32, -1.1, 1.1)
    base = jnp.clip(jax.random.normal(key_base, (SEQS, LEN, N_TP, D // N_TP), jnp.float32), -6.0, 6.0)
    return (base * jnp.exp(blocks)).reshape(SEQS, LEN, D).astype(jnp.bfloat16)


def block_scale(key, extent, cuts, low, top_value):
    loudness = 1.0
    for axis_at, shards_of in cuts:
        draws = jax.random.uniform(jax.random.fold_in(jax.random.fold_in(key, 6), axis_at), (shards_of,), jnp.float32, low / len(cuts), top_value / len(cuts))
        loudness = loudness * jnp.repeat(jnp.exp(draws), extent[axis_at] // shards_of).reshape((-1,) + (1,) * (len(extent) - 1 - axis_at))
    return loudness


def normal_values(stream_key, dims, scale, bound, shards=(), held_as=jnp.bfloat16):
    result = jax.random.normal(stream_key, dims, jnp.float32) * scale
    if len(shards) > 0:
        result = block_scale(stream_key, dims, shards, -0.22, 0.18) * result
    return jnp.clip(result, min=-bound, max=bound).astype(held_as)


def setup_inputs(seed: int = 0) -> dict:
    keys = jax.random.split(jax.random.key(seed), 16)
    return {
        "tokens": draw_tokens(jax.random.fold_in(keys[15], 71), 0),
        "first_gain": jnp.clip(1.0 + 0.18 * jax.random.normal(keys[1], (D,), jnp.float32), 0.1, 1.9),
        "first_gate": normal_values(keys[2], (D, FF), D ** -0.5, 0.125, ((0, 16), (1, 8))),
        "first_up": normal_values(keys[3], (D, FF), D ** -0.5, 0.125, ((0, 16), (1, 8))),
        "first_down": normal_values(keys[4], (FF, D), FF ** -0.5, 0.078125, ((0, 8), (1, 16))),
        "mixer_gain": jnp.clip(1.0 + 0.18 * jax.random.normal(keys[5], (D,), jnp.float32), 0.1, 1.9),
        "conv_input": normal_values(keys[6], (D, CW), D ** -0.5, 0.125, ((0, 16), (1, 8))),
        "outer_gate": normal_values(keys[7], (D, CW), D ** -0.5, 0.125, ((0, 16), (1, 8))),
        "inner_gate": normal_values(keys[8], (D, CW), D ** -0.5, 0.125, ((0, 16), (1, 8))),
        "conv_taps": normal_values(keys[9], (KERNEL, CW), KERNEL ** -0.5, 3.5, ((1, 8),), jnp.float32),
        "mixer_out": normal_values(keys[10], (CW, D), CW ** -0.5, 0.1875, ((0, 8), (1, 16))),
        "second_gain": jnp.clip(1.0 + 0.18 * jax.random.normal(keys[11], (D,), jnp.float32), 0.1, 1.9),
        "second_gate": normal_values(keys[12], (D, FF), D ** -0.5, 0.125, ((0, 16), (1, 8))),
        "second_up": normal_values(keys[13], (D, FF), D ** -0.5, 0.125, ((0, 16), (1, 8))),
        "second_down": normal_values(keys[14], (FF, D), FF ** -0.5, 0.078125, ((0, 8), (1, 16))),
    }


epsilon = 1e-05

def norm_rows(stream, gain):
    values = stream.astype(jnp.float32)
    scale = lax.rsqrt(lax.optimization_barrier(jnp.mean(values * values, axis=1, keepdims=True)) + epsilon)
    return (values * scale * gain).astype(jnp.bfloat16)

def block_sum(hidden, weight):
    count, inner = hidden.shape
    width = inner // N_TP
    hidden_blocks = hidden.reshape(count, N_TP, width).transpose(1, 0, 2)
    weight_blocks = weight.reshape(N_TP, width, weight.shape[1])

    def add_block(total, pair):
        part = jnp.dot(pair[0], pair[1], preferred_element_type=jnp.float32).astype(jnp.bfloat16)
        part = lax.optimization_barrier(part)
        return (total + part.astype(jnp.float32), None)
    start = jnp.zeros((count, weight.shape[1]), jnp.float32)
    total, _ = lax.scan(add_block, start, (hidden_blocks, weight_blocks))
    return total

def half_ffn(stream, gain, gate_weight, up_weight, down_weight):
    normed = norm_rows(stream, gain)
    gate = jnp.dot(normed, gate_weight, preferred_element_type=jnp.float32)
    upward = jnp.dot(normed, up_weight, preferred_element_type=jnp.float32)
    hidden = (jax.nn.silu(gate) * upward).astype(jnp.bfloat16)
    branch = block_sum(hidden, down_weight)
    return (stream.astype(jnp.float32) + 0.5 * branch).astype(jnp.bfloat16)

def conv_mixer(stream, seqs, gain, conv_input, outer_gate, inner_gate, conv_taps, mixer_out):
    normed = norm_rows(stream, gain)
    conv_values = jnp.dot(normed, conv_input, preferred_element_type=jnp.float32)
    outer = jnp.dot(normed, outer_gate, preferred_element_type=jnp.float32)
    inner = jnp.dot(normed, inner_gate, preferred_element_type=jnp.float32)
    gated_input = (inner * conv_values).reshape(seqs, -1, conv_values.shape[1])
    one_back = jnp.pad(gated_input, ((0, 0), (1, 0), (0, 0)))[:, :-1]
    two_back = jnp.pad(gated_input, ((0, 0), (2, 0), (0, 0)))[:, :-2]
    convolved = conv_taps[0] * two_back + conv_taps[1] * one_back + conv_taps[2] * gated_input
    mixed = (outer * convolved.reshape(conv_values.shape)).astype(jnp.bfloat16)
    branch = block_sum(mixed, mixer_out)
    return (stream.astype(jnp.float32) + branch).astype(jnp.bfloat16)

def reference(tokens, first_gain, first_gate, first_up, first_down, mixer_gain, conv_input, outer_gate, inner_gate, conv_taps, mixer_out, second_gain, second_gate, second_up, second_down):
    seqs, length, width = tokens.shape
    stream = tokens.reshape(seqs * length, width)
    stream = half_ffn(stream, first_gain, first_gate, first_up, first_down)
    stream = conv_mixer(stream, seqs, mixer_gain, conv_input, outer_gate, inner_gate, conv_taps, mixer_out)
    stream = half_ffn(stream, second_gain, second_gate, second_up, second_down)
    return stream.reshape(seqs, length, width)
```

```python
import functools

import jax
import jax.numpy as jnp
from jax import lax
from jax.experimental import pallas as pl
from jax.experimental.pallas import tpu as pltpu
from jax.sharding import PartitionSpec as P

EPS = 1e-05
MESH = pl.DeviceIdType.MESH
F32, BF16 = jnp.float32, jnp.bfloat16

D = 2048
ROWS = 768
LEN = 384
BLK = 256
NC = 2
R = ROWS // NC
HALF = R // 2
SUB = 64
SLABS = 34
GROUPS = ((0, 10), (10, 5), (15, 4), (19, 10), (29, 5))
UNITS = (0, 2, 3, 4, 3, 2, 1)
AHEAD = (2, 1, 3, 0)


def schedule():
    order = [("W", 0, 0), ("G0", 0, 0), ("G0", 0, 1), ("W", 0, 1), ("G1", 0, 0), ("G1", 0, 1), ("W", 0, 2)]
    order += [("G2", 0, 0), ("G2", 0, 1), ("G3", 0, 0), ("N", 0, 0), ("G3", 0, 1), ("N", 0, 1)]
    order += [("W", 0, 3), ("W", 1, 0), ("W", 0, 4), ("W", 0, 5), ("W", 1, 1), ("F", 0, 0), ("W", 1, 2), ("F", 0, 1)]
    order += [("W", 1, 3), ("W", 2, 0), ("W", 1, 4), ("W", 1, 5), ("W", 2, 1)]
    order += [("DP", 0, 0), ("DO", 0, 0), ("SA", 0, 0), ("DP", 0, 1), ("DO", 0, 1), ("SA", 0, 1), ("W", 2, 2)]
    order += [("SB", 0, 0), ("SB", 0, 1), ("W", 2, 3), ("W", 3, 0), ("SC", 0, 0), ("W", 2, 4), ("SC", 0, 1), ("W", 2, 5)]
    order += [("G1", 1, 0), ("W", 3, 1), ("G2", 1, 0), ("G1", 1, 1), ("G3", 1, 0), ("N", 1, 0), ("F", 1, 0), ("DP", 1, 0)]
    order += [("DO", 1, 0), ("SA", 1, 0), ("G2", 1, 1), ("G3", 1, 1), ("N", 1, 1), ("F", 1, 1), ("SB", 1, 0), ("DP", 1, 1)]
    order += [("W", 3, 2), ("DO", 1, 1), ("SA", 1, 1), ("SC", 1, 0), ("SB", 1, 1), ("W", 3, 3), ("W", 4, 0), ("G1", 2, 0)]
    order += [("SC", 1, 1), ("G2", 2, 0), ("W", 3, 4), ("G1", 2, 1), ("G3", 2, 0), ("N", 2, 0), ("G2", 2, 1), ("W", 3, 5)]
    order += [("W", 4, 1), ("F", 2, 0), ("G3", 2, 1), ("N", 2, 1), ("F", 2, 1), ("W", 4, 2), ("W", 4, 3), ("W", 4, 4), ("W", 4, 5)]
    order += [("DP", 2, 0), ("DO", 2, 0), ("SA", 2, 0), ("DP", 2, 1), ("DO", 2, 1), ("SA", 2, 1)]
    order += [("SB", 2, 0), ("SB", 2, 1), ("SC", 2, 0), ("SC", 2, 1)]
    return order


def layer_kernel(
    tokens, gains, taps, fgate, fup, fdown, conv_in, outer_gate, inner_gate, mix_out, sgate, sup, sdown,
    out,
    w, xg, normed, hidden, psend, precv, pown, s1, r1, s2, r2, gi, outer_s, mixed, result,
    w_load, x_load, w_send, w_recv, y_send, g_recv, s_recv, o_sem,
):
    f, t = lax.axis_index("fs"), lax.axis_index("tp")
    z, x = f // 4, f % 4
    y, core = t // 2, t % 2
    other = 1 - core

    def slot(h, a, b):
        za, xa = (b, a) if h == 0 else (a, b)
        return ((z + za) % 4) * 4 + (x + xa) % 4

    def at_y(ahead, which):
        return ((y + ahead) % 4) * 2 + which

    def w_device(h, phase, d):
        return (slot(h, d, 0) if phase == 1 else slot(h, 0, d), t)

    up, down, partner = (f, at_y(1, core)), (f, at_y(3, core)), (f, at_y(0, other))

    def load_tokens():
        return pltpu.make_async_copy(tokens, xg.at[0, t], x_load)

    def loads(g):
        sources = []
        if g in (0, 3):
            for s in range(5):
                for a in (fgate, fup) if g == 0 else (sgate, sup):
                    sources.append(a.at[:, pl.ds(128 * s, 128)])
        elif g in (1, 4):
            a = fdown if g == 1 else sdown
            sources = [a.at[pl.ds(128 * s, 128), :] for s in range(5)]
        else:
            sources = [conv_in, outer_gate, inner_gate, mix_out]
        first = GROUPS[g][0]
        return [pltpu.make_async_copy(a, w.at[f, first + i], w_load.at[g]) for i, a in enumerate(sources)]

    def await_bytes(ref, sem):
        pltpu.make_async_copy(ref, ref, sem).wait()

    load_tokens().start()
    for g in range(5):
        for copy in loads(g):
            copy.start()

    barrier = pltpu.get_barrier_semaphore()
    peers = [w_device(h, 1, d) for h in (0, 1) for d in (1, 3)] + [up, down, partner]
    for peer in peers:
        pl.semaphore_signal(barrier, inc=1, device_id=peer, device_id_type=MESH)

    gi[:, pl.ds(0, 8), :] = jnp.zeros((2, 8, 128), F32)

    load_tokens().wait()
    pl.semaphore_wait(barrier, len(peers))

    def w_copy(g, h, a, b, phase, d, quarter, landing):
        first, count = GROUPS[g]
        if quarter:
            rows = pl.ds(64 * h + (0 if d == 1 else 32), 32)
        else:
            rows = pl.ds(64 * h, 64)
        part = w.at[slot(h, a, b), pl.ds(first, count), rows]
        pltpu.make_async_remote_copy(
            src_ref=part, dst_ref=part, send_sem=w_send.at[g], recv_sem=w_recv.at[g, landing],
            device_id=w_device(h, phase, d), device_id_type=MESH,
        ).start()

    def w_wait(g, landing):
        first, count = GROUPS[g]
        await_bytes(w.at[pl.ds(0, UNITS[landing]), pl.ds(first, count)], w_recv.at[g, landing])

    both = [(h, d) for h in (0, 1) for d in (1, 3)]

    def weights(g, rnd):
        first, count = GROUPS[g]
        if rnd == 0:
            await_bytes(w.at[f, pl.ds(first, count)], w_load.at[g])
            for h, d in both:
                w_copy(g, h, 0, 0, 1, d, False, 1)
            for h, d in both:
                w_copy(g, h, 0, 0, 2, d, False, 2)
        elif rnd == 5:
            w_wait(g, 5)
            w_wait(g, 6)
        else:
            w_wait(g, rnd)
            for h, d in both:
                back = 4 - d
                if rnd == 1:
                    w_copy(g, h, back, 0, 1, d, True, 2)
                    w_copy(g, h, 1, 0, 2, d, False, 3)
                    w_copy(g, h, 3, 0, 2, d, False, 3)
                elif rnd == 2:
                    w_copy(g, h, 0, back, 2, d, True, 4)
                    w_copy(g, h, 2, 0, 2, d, False, 4)
                elif rnd == 3:
                    w_copy(g, h, 1, back, 2, d, True, 5)
                    w_copy(g, h, 3, back, 2, d, True, 5)
                else:
                    w_copy(g, h, 2, back, 2, d, True, 6)

    def y_copy(src, dst, stage, c, recv, device):
        pltpu.make_async_remote_copy(
            src_ref=src, dst_ref=dst, send_sem=y_send.at[stage, c], recv_sem=recv,
            device_id=device, device_id_type=MESH,
        ).start()

    def rows_of(c):
        return pl.ds(c * R, R)

    def front(c):
        return pl.ds(c * R, HALF)

    def rear(c):
        return pl.ds(c * R + HALF, HALF)

    def gather_0(stage, c):
        mine = xg.at[stage, t, rows_of(c)]
        for device in (up, down):
            y_copy(mine, mine, stage, c, g_recv.at[stage, c, 0], device)
        y_copy(mine, mine, stage, c, g_recv.at[stage, c, 2], partner)

    def gather_1(stage, c):
        await_bytes(xg.at[stage, pl.ds(0, 2), rows_of(c)], g_recv.at[stage, c, 0])
        below, above = at_y(3, core), at_y(1, core)
        for block, part, device in ((below, front(c), up), (above, rear(c), down)):
            ref = xg.at[stage, block, part]
            y_copy(ref, ref, stage, c, g_recv.at[stage, c, 1], device)
        for block in (below, above):
            ref = xg.at[stage, block, rows_of(c)]
            y_copy(ref, ref, stage, c, g_recv.at[stage, c, 2], partner)

    def gather_2(stage, c):
        await_bytes(xg.at[stage, 0, rows_of(c)], g_recv.at[stage, c, 1])
        ref = xg.at[stage, at_y(2, core), rows_of(c)]
        y_copy(ref, ref, stage, c, g_recv.at[stage, c, 2], partner)

    def gather_3(stage, c):
        await_bytes(xg.at[stage, pl.ds(0, 4), rows_of(c)], g_recv.at[stage, c, 2])

    def norm(stage, c):
        @pl.loop(0, R // SUB)
        def _(i):
            rows = pl.ds(pl.multiple_of(c * R + i * SUB, SUB), SUB)
            total = jnp.zeros((SUB, BLK), F32)
            for b in range(8):
                v = xg[stage, b, rows, :].astype(F32)
                total = total + v * v
            mean = jnp.sum(total, axis=1, keepdims=True) * (1.0 / D)
            scale = lax.rsqrt(mean + EPS)
            for b in range(8):
                v = xg[stage, b, rows, :].astype(F32)
                cols = pl.ds(b * BLK, BLK)
                normed[rows, cols] = (v * scale * gains[stage : stage + 1, cols]).astype(BF16)

    def columns(first):
        return w[:, first].reshape(D, 128)

    def ffn(stage, c):
        first = 0 if stage == 0 else 19

        @pl.loop(0, 5)
        def _(s):
            pair = jnp.concatenate([columns(first + 2 * s), columns(first + 2 * s + 1)], axis=1)
            both_halves = jnp.dot(normed[rows_of(c), :], pair, preferred_element_type=F32)
            gate, upward = both_halves[:, :128], both_halves[:, 128:]
            value = gate / (1.0 + jnp.exp(-gate)) * upward
            hidden[rows_of(c), pl.ds(pl.multiple_of(128 * s, 128), 128)] = value.astype(BF16)

    def mixer(c):
        three = jnp.concatenate([columns(15), columns(16), columns(17)], axis=1)
        products = jnp.dot(normed[rows_of(c), :], three, preferred_element_type=F32)
        seq, at = c * R // LEN, c * R % LEN
        gi[seq, pl.ds(8 + at, R), :] = products[:, 256:] * products[:, :128]
        outer_s[...] = products[:, 128:256]
        convolved = taps[0:1, :] * gi[seq, pl.ds(6 + at, R), :]
        convolved = convolved + taps[1:2, :] * gi[seq, pl.ds(7 + at, R), :]
        convolved = convolved + taps[2:3, :] * gi[seq, pl.ds(8 + at, R), :]
        mixed[rows_of(c), :] = (outer_s[...] * convolved).astype(BF16)

    def product(stage, c, block):
        a, b = 2 * block, 2 * block + 1
        if stage == 1:
            pair = jnp.concatenate([w[a, 18], w[b, 18]], axis=1)
            return jnp.dot(mixed[rows_of(c), :], pair, preferred_element_type=F32)
        slabs = pl.ds(10 if stage == 0 else 29, 5)
        pair = jnp.concatenate([w[a, slabs].reshape(640, 128), w[b, slabs].reshape(640, 128)], axis=1)
        return jnp.dot(hidden[rows_of(c), :], pair, preferred_element_type=F32)

    def down_partner(stage, c):
        for i in range(4):
            psend[stage, i, rows_of(c), :] = product(stage, c, at_y(AHEAD[i], other)).astype(BF16)
        part = pl.ds(0, 4)
        y_copy(psend.at[stage, part, rows_of(c)], precv.at[stage, part, rows_of(c)], stage, c, s_recv.at[stage, c, 0], partner)

    def down_own(stage, c):
        for i in range(4):
            pown[i, rows_of(c), :] = product(stage, c, at_y(AHEAD[i], core))

    def pair_sum(stage, i, rows):
        return pown[i, rows, :] + precv[stage, i, rows, :].astype(F32)

    def over(first, count, body):
        @pl.loop(0, count // SUB)
        def _(i):
            body(pl.ds(pl.multiple_of(first + i * SUB, SUB), SUB))

    def sum_a(stage, c):
        await_bytes(precv.at[stage, pl.ds(0, 4), rows_of(c)], s_recv.at[stage, c, 0])

        def body(rows):
            s1[stage, rows, :] = pair_sum(stage, 0, rows).astype(BF16)

        over(c * R, R, body)
        for part, device in ((front(c), up), (rear(c), down)):
            y_copy(s1.at[stage, part], r1.at[stage, part], stage, c, s_recv.at[stage, c, 1], device)

    def sum_b(stage, c):
        await_bytes(r1.at[stage, rows_of(c)], s_recv.at[stage, c, 1])

        def with_r1(i, rows):
            value = pair_sum(stage, i, rows) + r1[stage, rows, :].astype(F32)
            s2[stage, i - 1, rows, :] = value.astype(BF16)

        def alone(i, rows):
            s2[stage, i - 1, rows, :] = pair_sum(stage, i, rows).astype(BF16)

        def front_body(rows):
            with_r1(1, rows)
            alone(2, rows)

        def rear_body(rows):
            alone(1, rows)
            with_r1(2, rows)

        over(c * R, HALF, front_body)
        over(c * R + HALF, HALF, rear_body)
        for i, device in ((0, up), (1, down)):
            y_copy(s2.at[stage, i, rows_of(c)], r2.at[stage, i, rows_of(c)], stage, c, s_recv.at[stage, c, 2], device)

    def sum_c(stage, c):
        await_bytes(r2.at[stage, pl.ds(0, 2), rows_of(c)], s_recv.at[stage, c, 2])

        def body(rows):
            branch = pair_sum(stage, 3, rows) + r2[stage, 0, rows, :].astype(F32) + r2[stage, 1, rows, :].astype(F32)
            if stage != 1:
                branch = 0.5 * branch
            value = (xg[stage, t, rows, :].astype(F32) + branch).astype(BF16)
            if stage < 2:
                xg[stage + 1, t, rows, :] = value
            else:
                result[rows, :] = value

        over(c * R, R, body)
        if stage < 2:
            gather_0(stage + 1, c)
        else:
            pltpu.make_async_copy(result.at[rows_of(c)], out.at[rows_of(c)], o_sem.at[c]).start()

    def mid(stage, c):
        if stage == 1:
            mixer(c)
        else:
            ffn(stage, c)

    tasks = dict(
        W=weights, G0=gather_0, G1=gather_1, G2=gather_2, G3=gather_3, N=norm, F=mid,
        DP=down_partner, DO=down_own, SA=sum_a, SB=sum_b, SC=sum_c,
    )
    for name, a, b in schedule():
        with jax.named_scope(f"{name}_{a}_{b}"):
            tasks[name](a, b)

    for c in range(NC):
        pltpu.make_async_copy(result.at[rows_of(c)], out.at[rows_of(c)], o_sem.at[c]).wait()
    for g, (first, count) in enumerate(GROUPS):
        await_bytes(w.at[pl.ds(0, 15), pl.ds(first, count)], w_send.at[g])
    for stage in range(3):
        for c in range(NC):
            await_bytes(xg.at[0, pl.ds(0, 7), rows_of(c)], y_send.at[stage, c])
            await_bytes(xg.at[0, pl.ds(0, 7), rows_of(c)], y_send.at[stage, c])


def on_device(
    tokens, first_gain, first_gate, first_up, first_down, mixer_gain, conv_input, outer_gate, inner_gate, conv_taps,
    mixer_out, second_gain, second_gate, second_up, second_down,
):
    shape = tokens.shape
    gains = jnp.stack([first_gain, mixer_gain, second_gain])
    hbm, vmem = pl.BlockSpec(memory_space=pl.ANY), pl.BlockSpec(memory_space=pltpu.VMEM)
    dma = pltpu.SemaphoreType.DMA
    result = pl.pallas_call(
        layer_kernel,
        out_shape=jax.ShapeDtypeStruct((ROWS, BLK), BF16),
        in_specs=[hbm, vmem, vmem] + [hbm] * 10,
        out_specs=hbm,
        scratch_shapes=[
            pltpu.VMEM((16, SLABS, 128, 128), BF16),
            pltpu.VMEM((3, 8, ROWS, BLK), BF16),
            pltpu.VMEM((ROWS, D), BF16),
            pltpu.VMEM((ROWS, 640), BF16),
            pltpu.VMEM((3, 4, ROWS, BLK), BF16),
            pltpu.VMEM((3, 4, ROWS, BLK), BF16),
            pltpu.VMEM((4, ROWS, BLK), F32),
            pltpu.VMEM((3, ROWS, BLK), BF16),
            pltpu.VMEM((3, ROWS, BLK), BF16),
            pltpu.VMEM((3, 2, ROWS, BLK), BF16),
            pltpu.VMEM((3, 2, ROWS, BLK), BF16),
            pltpu.VMEM((2, 8 + LEN, 128), F32),
            pltpu.VMEM((R, 128), F32),
            pltpu.VMEM((ROWS, 128), BF16),
            pltpu.VMEM((ROWS, BLK), BF16),
            dma((5,)),
            dma,
            dma((5,)),
            dma((5, 7)),
            dma((3, NC)),
            dma((3, NC, 3)),
            dma((3, NC, 3)),
            dma((NC,)),
        ],
        compiler_params=pltpu.CompilerParams(
            collective_id=0, has_side_effects=True, vmem_limit_bytes=67_000_000
        ),
    )(
        tokens.reshape(ROWS, BLK), gains, conv_taps, first_gate, first_up, first_down, conv_input, outer_gate,
        inner_gate, mixer_out, second_gate, second_up, second_down,
    )
    return result.reshape(shape)


def solution(mesh):
    fs, tp = P("fs", "tp"), P("tp", "fs")
    in_specs = (
        P("fs", None, "tp"), P(), fs, fs, tp, P(), fs, fs, fs, P(None, "tp"), tp, P(), fs, fs, tp,
    )
    return jax.shard_map(
        on_device, mesh=mesh, in_specs=in_specs, out_specs=P("fs", None, "tp"), check_vma=False
    )
```

```python
import functools

import jax
import jax.numpy as jnp
from jax import lax
from jax.experimental import pallas as pl
from jax.experimental.pallas import tpu as pltpu
from jax.sharding import PartitionSpec as P

EPS = 1e-05
MESH = pl.DeviceIdType.MESH
F32, BF16 = jnp.float32, jnp.bfloat16

D = 2048
ROWS = 768
LEN = 384
BLK = 256
NC = 4
R = ROWS // NC
HALF = R // 2
SUB = 96
SLABS = 34
GROUPS = ((0, 10), (10, 5), (15, 4), (19, 10), (29, 5))
UNITS = (0, 2, 3, 4, 3, 2, 1)
AHEAD = (2, 1, 3, 0)


ORDER = (
    ("W", 0, 0), ("G0", 0, 1), ("W", 1, 0), ("W", 0, 1), ("G0", 0, 0), ("G0", 0, 2), ("G1", 0, 2), ("G1", 0, 1),
    ("W", 0, 2), ("G2", 0, 1), ("G0", 0, 3), ("G1", 0, 0), ("G2", 0, 2), ("G1", 0, 3), ("W", 1, 1), ("W", 1, 2),
    ("G3", 0, 2), ("G3", 0, 1), ("W", 0, 3), ("W", 0, 4), ("W", 1, 3), ("G2", 0, 0), ("W", 1, 4), ("W", 2, 0),
    ("G2", 0, 3), ("G3", 0, 3), ("G3", 0, 0), ("N", 0, 0), ("N", 0, 2), ("N", 0, 3), ("W", 3, 0), ("N", 0, 1),
    ("W", 0, 5), ("F", 0, 0), ("F", 0, 1), ("W", 1, 5), ("DA", 0, 1), ("DA", 0, 0), ("F", 0, 2), ("SA", 0, 1),
    ("DA", 0, 2), ("DB", 0, 1), ("SA", 0, 0), ("W", 2, 1), ("DB", 0, 0), ("SA", 0, 2), ("SB", 0, 1), ("F", 0, 3),
    ("DA", 0, 3), ("SB", 0, 0), ("DB", 0, 3), ("SA", 0, 3), ("W", 2, 2), ("SC", 0, 1), ("DB", 0, 2), ("W", 4, 0),
    ("SC", 0, 0), ("SB", 0, 2), ("W", 2, 3), ("W", 2, 4), ("G1", 1, 0), ("G1", 1, 1), ("W", 3, 1), ("SB", 0, 3),
    ("SC", 0, 2), ("G2", 1, 0), ("G2", 1, 1), ("W", 2, 5), ("W", 4, 1), ("G3", 1, 0), ("N", 1, 0), ("SC", 0, 3),
    ("F", 1, 0), ("DA", 1, 0), ("G3", 1, 1), ("N", 1, 1), ("F", 1, 1), ("DA", 1, 1), ("G1", 1, 2), ("SA", 1, 0),
    ("W", 3, 2), ("DB", 1, 0), ("DB", 1, 1), ("G1", 1, 3), ("G2", 1, 2), ("SA", 1, 1), ("SB", 1, 0), ("G2", 1, 3),
    ("G3", 1, 2), ("N", 1, 2), ("SB", 1, 1), ("W", 4, 2), ("W", 3, 3), ("F", 1, 2), ("DA", 1, 2), ("G3", 1, 3),
    ("SC", 1, 0), ("N", 1, 3), ("F", 1, 3), ("DA", 1, 3), ("SA", 1, 2), ("SC", 1, 1), ("DB", 1, 2), ("SA", 1, 3),
    ("G1", 2, 0), ("SB", 1, 2), ("W", 3, 4), ("W", 4, 3), ("DB", 1, 3), ("W", 4, 4), ("G1", 2, 1), ("SB", 1, 3),
    ("G2", 2, 0), ("G3", 2, 0), ("SC", 1, 2), ("G2", 2, 1), ("N", 2, 0), ("W", 3, 5), ("F", 2, 0), ("SC", 1, 3),
    ("G3", 2, 1), ("N", 2, 1), ("W", 4, 5), ("DA", 2, 0), ("DB", 2, 0), ("G1", 2, 2), ("F", 2, 1), ("SA", 2, 0),
    ("DA", 2, 1), ("G1", 2, 3), ("G2", 2, 2), ("DB", 2, 1), ("SA", 2, 1), ("SB", 2, 0), ("G3", 2, 2), ("G2", 2, 3),
    ("N", 2, 2), ("F", 2, 2), ("DA", 2, 2), ("SB", 2, 1), ("G3", 2, 3), ("N", 2, 3), ("F", 2, 3), ("DA", 2, 3),
    ("SA", 2, 2), ("DB", 2, 2), ("DB", 2, 3), ("SA", 2, 3), ("SB", 2, 2), ("SC", 2, 0), ("SB", 2, 3), ("SC", 2, 1),
    ("SC", 2, 2), ("SC", 2, 3),
)


def layer_kernel(
    tokens, gain_1, gain_2, gain_3, taps_in, fgate, fup, fdown, conv_in, outer_gate, inner_gate, mix_out, sgate, sup, sdown,
    out,
    w, xg, normed, hidden, psend, precv, pown, s1, r1, s2, r2, gi, outer_s, mixed, result, gains, taps,
    w_load, x_load, w_send, w_recv, y_send, g_recv, s_recv, o_sem, k_load,
):
    f, t = lax.axis_index("fs"), lax.axis_index("tp")
    z, x = lax.div(f, 4), lax.rem(f, 4)
    y, core = lax.div(t, 2), lax.rem(t, 2)
    other = 1 - core
    zs = [4 * lax.rem(z + i, 4) for i in range(4)]
    xs = [lax.rem(x + i, 4) for i in range(4)]
    ys = [2 * lax.rem(y + i, 4) for i in range(4)]
    slots = [[zs[i] + xs[j] for j in range(4)] for i in range(4)]
    mine, others = [a + core for a in ys], [a + other for a in ys]

    def slot(h, a, b):
        return slots[b][a] if h == 0 else slots[a][b]

    def w_device(h, phase, d):
        return (slot(h, d, 0) if phase == 1 else slot(h, 0, d), t)

    above, below, partner = (f, mine[1]), (f, mine[3]), (f, others[0])

    def load_tokens():
        return pltpu.make_async_copy(tokens, xg.at[0, t], x_load)

    def loads(g):
        sources = []
        if g in (0, 3):
            for s in range(5):
                for a in (fgate, fup) if g == 0 else (sgate, sup):
                    sources.append(a.at[:, pl.ds(128 * s, 128)])
        elif g in (1, 4):
            a = fdown if g == 1 else sdown
            sources = [a.at[pl.ds(128 * s, 128), :] for s in range(5)]
        else:
            sources = [conv_in, outer_gate, inner_gate, mix_out]
        first = GROUPS[g][0]
        return [pltpu.make_async_copy(a, w.at[f, first + i], w_load.at[g]) for i, a in enumerate(sources)]

    def await_bytes(ref, sem):
        pltpu.make_async_copy(ref, ref, sem).wait()

    def load_vectors():
        copies = [pltpu.make_async_copy(a, gains.at[i], k_load.at[i]) for i, a in enumerate((gain_1, gain_2, gain_3))]
        return copies + [pltpu.make_async_copy(taps_in, taps, k_load.at[3])]

    load_tokens().start()
    for g in range(5):
        for copy in loads(g):
            copy.start()
    for copy in load_vectors():
        copy.start()

    barrier = pltpu.get_barrier_semaphore()
    peers = [w_device(h, 1, d) for h in (0, 1) for d in (1, 3)] + [above, below, partner]
    for peer in peers:
        pl.semaphore_signal(barrier, inc=1, device_id=peer, device_id_type=MESH)

    gi[:, pl.ds(0, 8), :] = jnp.zeros((2, 8, 128), F32)

    load_tokens().wait()
    for copy in load_vectors():
        copy.wait()
    pl.semaphore_wait(barrier, len(peers))

    def w_copy(g, h, a, b, phase, d, quarter, landing):
        first, count = GROUPS[g]
        if quarter:
            rows = pl.ds(64 * h + (0 if d == 1 else 32), 32)
        else:
            rows = pl.ds(64 * h, 64)
        part = w.at[slot(h, a, b), pl.ds(first, count), rows]
        pltpu.make_async_remote_copy(
            src_ref=part, dst_ref=part, send_sem=w_send.at[g], recv_sem=w_recv.at[g, landing],
            device_id=w_device(h, phase, d), device_id_type=MESH,
        ).start()

    def w_wait(g, landing):
        first, count = GROUPS[g]
        await_bytes(w.at[pl.ds(0, UNITS[landing]), pl.ds(first, count)], w_recv.at[g, landing])

    both = [(h, d) for h in (0, 1) for d in (1, 3)]

    def weights(g, rnd):
        first, count = GROUPS[g]
        if rnd == 0:
            await_bytes(w.at[f, pl.ds(first, count)], w_load.at[g])
            for h, d in both:
                w_copy(g, h, 0, 0, 1, d, False, 1)
            for h, d in both:
                w_copy(g, h, 0, 0, 2, d, False, 2)
        elif rnd == 5:
            w_wait(g, 5)
            w_wait(g, 6)
        else:
            w_wait(g, rnd)
            for h, d in both:
                back = 4 - d
                if rnd == 1:
                    w_copy(g, h, back, 0, 1, d, True, 2)
                elif rnd == 2:
                    w_copy(g, h, 0, back, 2, d, True, 4)
                elif rnd == 3:
                    w_copy(g, h, 1, back, 2, d, True, 5)
                    w_copy(g, h, 3, back, 2, d, True, 5)
                else:
                    w_copy(g, h, 2, back, 2, d, True, 6)
            for h, d in both:
                if rnd == 1:
                    w_copy(g, h, 1, 0, 2, d, False, 3)
                    w_copy(g, h, 3, 0, 2, d, False, 3)
                elif rnd == 2:
                    w_copy(g, h, 2, 0, 2, d, False, 4)

    def y_copy(src, dst, stage, c, recv, device):
        pltpu.make_async_remote_copy(
            src_ref=src, dst_ref=dst, send_sem=y_send.at[stage, c], recv_sem=recv,
            device_id=device, device_id_type=MESH,
        ).start()

    def rows_of(c):
        return pl.ds(c * R, R)

    def front(c):
        return pl.ds(c * R, HALF)

    def rear(c):
        return pl.ds(c * R + HALF, HALF)

    def gather_0(stage, c):
        ref = xg.at[stage, t, rows_of(c)]
        for device in (above, below):
            y_copy(ref, ref, stage, c, g_recv.at[stage, c, 0], device)
        y_copy(ref, ref, stage, c, g_recv.at[stage, c, 2], partner)

    def gather_1(stage, c):
        await_bytes(xg.at[stage, pl.ds(0, 2), rows_of(c)], g_recv.at[stage, c, 0])
        blocks = mine[3], mine[1]
        for block, part, device in ((blocks[0], front(c), above), (blocks[1], rear(c), below)):
            ref = xg.at[stage, block, part]
            y_copy(ref, ref, stage, c, g_recv.at[stage, c, 1], device)
        for block in blocks:
            ref = xg.at[stage, block, rows_of(c)]
            y_copy(ref, ref, stage, c, g_recv.at[stage, c, 2], partner)

    def gather_2(stage, c):
        await_bytes(xg.at[stage, 0, rows_of(c)], g_recv.at[stage, c, 1])
        ref = xg.at[stage, mine[2], rows_of(c)]
        y_copy(ref, ref, stage, c, g_recv.at[stage, c, 2], partner)

    def gather_3(stage, c):
        await_bytes(xg.at[stage, pl.ds(0, 4), rows_of(c)], g_recv.at[stage, c, 2])

    def norm(stage, c):
        @pl.loop(0, R // SUB)
        def _(i):
            rows = pl.ds(pl.multiple_of(c * R + i * SUB, SUB), SUB)
            total = jnp.zeros((SUB, BLK), F32)
            for b in range(8):
                v = xg[stage, b, rows, :].astype(F32)
                total = total + v * v
            mean = jnp.sum(total, axis=1, keepdims=True) * (1.0 / D)
            scale = lax.rsqrt(mean + EPS)
            for b in range(8):
                v = xg[stage, b, rows, :].astype(F32)
                cols = pl.ds(b * BLK, BLK)
                normed[rows, cols] = (v * scale * gains[stage, :, cols]).astype(BF16)

    def columns(first):
        return w[:, first].reshape(D, 128)

    def ffn(stage, c):
        first = 0 if stage == 0 else 19

        all_columns = jnp.concatenate([columns(first + 2 * s + i) for i in (0, 1) for s in range(5)], axis=1)
        products = jnp.dot(normed[rows_of(c), :], all_columns, preferred_element_type=F32)
        gate, upward = products[:, :640], products[:, 640:]
        hidden[rows_of(c), :] = (gate / (1.0 + jnp.exp(-gate)) * upward).astype(BF16)

    def mixer(c):
        three = jnp.concatenate([columns(15), columns(16), columns(17)], axis=1)
        products = jnp.dot(normed[rows_of(c), :], three, preferred_element_type=F32)
        seq, at = c * R // LEN, c * R % LEN
        gi[seq, pl.ds(8 + at, R), :] = products[:, 256:] * products[:, :128]
        outer_s[...] = products[:, 128:256]
        convolved = taps[0:1, :] * gi[seq, pl.ds(6 + at, R), :]
        convolved = convolved + taps[1:2, :] * gi[seq, pl.ds(7 + at, R), :]
        convolved = convolved + taps[2:3, :] * gi[seq, pl.ds(8 + at, R), :]
        mixed[rows_of(c), :] = (outer_s[...] * convolved).astype(BF16)

    def product(stage, c, blocks):
        if stage == 1:
            rows, columns = mixed[rows_of(c), :], [w[2 * b + i, 18] for b in blocks for i in (0, 1)]
        else:
            slabs = pl.ds(10 if stage == 0 else 29, 5)
            rows, columns = hidden[rows_of(c), :], [w[2 * b + i, slabs].reshape(640, 128) for b in blocks for i in (0, 1)]
        return jnp.dot(rows, jnp.concatenate(columns, axis=1), preferred_element_type=F32)

    def down(stage, c, first, count, landing):
        products = product(stage, c, [others[AHEAD[i]] for i in range(first, first + count)])
        for i in range(count):
            psend[stage, first + i, rows_of(c), :] = products[:, BLK * i : BLK * (i + 1)].astype(BF16)
        part = pl.ds(first, count)
        y_copy(psend.at[stage, part, rows_of(c)], precv.at[stage, part, rows_of(c)], stage, c, s_recv.at[stage, c, landing], partner)
        products = product(stage, c, [mine[AHEAD[i]] for i in range(first, first + count)])
        for i in range(count):
            pown[first + i, rows_of(c), :] = products[:, BLK * i : BLK * (i + 1)]

    def down_first(stage, c):
        down(stage, c, 0, 1, 0)

    def down_rest(stage, c):
        down(stage, c, 1, 3, 3)

    def pair_sum(stage, i, rows):
        return pown[i, rows, :] + precv[stage, i, rows, :].astype(F32)

    def over(first, count, body):
        body(pl.ds(first, count))

    def sum_a(stage, c):
        await_bytes(precv.at[stage, 0, rows_of(c)], s_recv.at[stage, c, 0])

        def body(rows):
            s1[stage, rows, :] = pair_sum(stage, 0, rows).astype(BF16)

        over(c * R, R, body)
        for part, device in ((front(c), above), (rear(c), below)):
            y_copy(s1.at[stage, part], r1.at[stage, part], stage, c, s_recv.at[stage, c, 1], device)

    def sum_b(stage, c):
        await_bytes(precv.at[stage, pl.ds(1, 3), rows_of(c)], s_recv.at[stage, c, 3])
        await_bytes(r1.at[stage, rows_of(c)], s_recv.at[stage, c, 1])

        def with_r1(i, rows):
            value = pair_sum(stage, i, rows) + r1[stage, rows, :].astype(F32)
            s2[stage, i - 1, rows, :] = value.astype(BF16)

        def alone(i, rows):
            s2[stage, i - 1, rows, :] = pair_sum(stage, i, rows).astype(BF16)

        def front_body(rows):
            with_r1(1, rows)
            alone(2, rows)

        def rear_body(rows):
            alone(1, rows)
            with_r1(2, rows)

        over(c * R, HALF, front_body)
        over(c * R + HALF, HALF, rear_body)
        for i, device in ((0, above), (1, below)):
            y_copy(s2.at[stage, i, rows_of(c)], r2.at[stage, i, rows_of(c)], stage, c, s_recv.at[stage, c, 2], device)

    def sum_c(stage, c):
        await_bytes(r2.at[stage, pl.ds(0, 2), rows_of(c)], s_recv.at[stage, c, 2])

        def body(rows):
            branch = pair_sum(stage, 3, rows) + r2[stage, 0, rows, :].astype(F32) + r2[stage, 1, rows, :].astype(F32)
            if stage != 1:
                branch = 0.5 * branch
            value = (xg[stage, t, rows, :].astype(F32) + branch).astype(BF16)
            if stage < 2:
                xg[stage + 1, t, rows, :] = value
            else:
                result[rows, :] = value

        over(c * R, R, body)
        if stage < 2:
            gather_0(stage + 1, c)
        else:
            pltpu.make_async_copy(result.at[rows_of(c)], out.at[rows_of(c)], o_sem.at[c]).start()

    def mid(stage, c):
        if stage == 1:
            mixer(c)
        else:
            ffn(stage, c)

    tasks = dict(
        W=weights, G0=gather_0, G1=gather_1, G2=gather_2, G3=gather_3, N=norm, F=mid,
        DA=down_first, DB=down_rest, SA=sum_a, SB=sum_b, SC=sum_c,
    )
    for name, a, b in ORDER:
        with jax.named_scope(f"{name}_{a}_{b}"):
            tasks[name](a, b)

    for c in range(NC):
        pltpu.make_async_copy(result.at[rows_of(c)], out.at[rows_of(c)], o_sem.at[c]).wait()
    for g, (first, count) in enumerate(GROUPS):
        await_bytes(w.at[pl.ds(0, 15), pl.ds(first, count)], w_send.at[g])
    for stage in range(3):
        for c in range(NC):
            await_bytes(xg.at[0, pl.ds(0, 7), rows_of(c)], y_send.at[stage, c])
            await_bytes(xg.at[0, pl.ds(0, 7), rows_of(c)], y_send.at[stage, c])


def on_device(
    tokens, first_gain, first_gate, first_up, first_down, mixer_gain, conv_input, outer_gate, inner_gate, conv_taps,
    mixer_out, second_gain, second_gate, second_up, second_down,
):
    shape = tokens.shape
    hbm = pl.BlockSpec(memory_space=pl.ANY)
    dma = pltpu.SemaphoreType.DMA
    result = pl.pallas_call(
        layer_kernel,
        out_shape=jax.ShapeDtypeStruct((ROWS, BLK), BF16),
        in_specs=[hbm] * 15,
        out_specs=hbm,
        scratch_shapes=[
            pltpu.VMEM((16, SLABS, 128, 128), BF16),
            pltpu.VMEM((3, 8, ROWS, BLK), BF16),
            pltpu.VMEM((ROWS, D), BF16),
            pltpu.VMEM((ROWS, 640), BF16),
            pltpu.VMEM((3, 4, ROWS, BLK), BF16),
            pltpu.VMEM((3, 4, ROWS, BLK), BF16),
            pltpu.VMEM((4, ROWS, BLK), F32),
            pltpu.VMEM((3, ROWS, BLK), BF16),
            pltpu.VMEM((3, ROWS, BLK), BF16),
            pltpu.VMEM((3, 2, ROWS, BLK), BF16),
            pltpu.VMEM((3, 2, ROWS, BLK), BF16),
            pltpu.VMEM((2, 8 + LEN, 128), F32),
            pltpu.VMEM((R, 128), F32),
            pltpu.VMEM((ROWS, 128), BF16),
            pltpu.VMEM((ROWS, BLK), BF16),
            pltpu.VMEM((3, 1, D), F32),
            pltpu.VMEM((3, 128), F32),
            dma((5,)),
            dma,
            dma((5,)),
            dma((5, 7)),
            dma((3, NC)),
            dma((3, NC, 3)),
            dma((3, NC, 4)),
            dma((NC,)),
            dma((4,)),
        ],
        compiler_params=pltpu.CompilerParams(
            collective_id=0, has_side_effects=True, vmem_limit_bytes=67_000_000
        ),
    )(
        tokens.reshape(ROWS, BLK), first_gain[None], mixer_gain[None], second_gain[None], conv_taps, first_gate, first_up, first_down, conv_input, outer_gate,
        inner_gate, mixer_out, second_gate, second_up, second_down,
    )
    return result.reshape(shape)


def solution(mesh):
    fs, tp = P("fs", "tp"), P("tp", "fs")
    in_specs = (
        P("fs", None, "tp"), P(), fs, fs, tp, P(), fs, fs, fs, P(None, "tp"), tp, P(), fs, fs, tp,
    )
    return jax.shard_map(
        on_device, mesh=mesh, in_specs=in_specs, out_specs=P("fs", None, "tp"), check_vma=False
    )
```

```python
import functools

import jax
import jax.numpy as jnp
from jax import lax
from jax.experimental import pallas as pl
from jax.experimental.pallas import tpu as pltpu
from jax.sharding import PartitionSpec as P

EPS = 1e-05
MESH = pl.DeviceIdType.MESH
F32, BF16 = jnp.float32, jnp.bfloat16

D = 2048
ROWS = 768
LEN = 384
BLK = 256
NC = 4
R = ROWS // NC
HALF = R // 2
SUB = 96
SLABS = 34
GROUPS = ((0, 10), (10, 5), (15, 4), (19, 10), (29, 5))
UNITS = (0, 2, 3, 4, 3, 2, 1)
AHEAD = (2, 1, 3, 0)


ORDER = (
    ("W", 0, 0), ("G0", 0, 2), ("G0", 0, 3), ("G1", 0, 2), ("G0", 0, 0), ("W", 0, 1), ("G1", 0, 0), ("GH", 0, 0),
    ("G1", 0, 3), ("W", 1, 0), ("W", 0, 2), ("G0", 0, 1), ("W", 0, 3), ("G1", 0, 1), ("GH", 0, 1), ("W", 1, 1),
    ("GH", 0, 2), ("G2", 0, 2), ("G3", 0, 2), ("G2", 0, 1), ("GH", 0, 3), ("G2", 0, 0), ("N", 0, 2), ("G2", 0, 3),
    ("G3", 0, 3), ("N", 0, 3), ("G3", 0, 0), ("N", 0, 0), ("W", 1, 2), ("W", 0, 4), ("G3", 0, 1), ("W", 1, 3),
    ("N", 0, 1), ("W", 1, 4), ("W", 2, 0), ("W", 3, 0), ("W", 0, 5), ("F", 0, 3), ("F", 0, 0), ("W", 1, 5),
    ("DA", 0, 0), ("DA", 0, 3), ("DB", 0, 3), ("DB", 0, 0), ("SA", 0, 0), ("SA", 0, 3), ("F", 0, 2), ("DA", 0, 2),
    ("SE", 0, 0), ("DB", 0, 2), ("W", 2, 1), ("SB", 0, 0), ("SE", 0, 3), ("SA", 0, 2), ("F", 0, 1), ("SE", 0, 2),
    ("W", 2, 2), ("SC", 0, 0), ("DA", 0, 1), ("SB", 0, 2), ("SB", 0, 3), ("W", 4, 0), ("G1", 1, 0), ("DB", 0, 1),
    ("W", 2, 3), ("SA", 0, 1), ("W", 2, 4), ("SC", 0, 2), ("W", 3, 1), ("SC", 0, 3), ("GH", 1, 0), ("G2", 1, 0),
    ("G1", 1, 2), ("SE", 0, 1), ("W", 2, 5), ("SB", 0, 1), ("G3", 1, 0), ("N", 1, 0), ("W", 4, 1), ("GH", 1, 2),
    ("F", 1, 0), ("DA", 1, 0), ("DB", 1, 0), ("G1", 1, 3), ("G2", 1, 2), ("SA", 1, 0), ("SC", 0, 1), ("GH", 1, 3),
    ("G2", 1, 3), ("G3", 1, 2), ("N", 1, 2), ("F", 1, 2), ("SE", 1, 0), ("DA", 1, 2), ("SB", 1, 0), ("DB", 1, 2),
    ("W", 3, 2), ("G3", 1, 3), ("N", 1, 3), ("G1", 1, 1), ("F", 1, 3), ("DA", 1, 3), ("W", 3, 3), ("SA", 1, 2),
    ("SE", 1, 2), ("DB", 1, 3), ("GH", 1, 1), ("SA", 1, 3), ("G2", 1, 1), ("SC", 1, 0), ("SE", 1, 3), ("W", 4, 2),
    ("G3", 1, 1), ("N", 1, 1), ("F", 1, 1), ("SB", 1, 3), ("DA", 1, 1), ("SB", 1, 2), ("G1", 2, 0), ("GH", 2, 0),
    ("DB", 1, 1), ("W", 3, 4), ("W", 4, 3), ("SA", 1, 1), ("SC", 1, 3), ("G2", 2, 0), ("SE", 1, 1), ("SB", 1, 1),
    ("W", 4, 4), ("G1", 2, 3), ("GH", 2, 3), ("G3", 2, 0), ("SC", 1, 2), ("N", 2, 0), ("W", 3, 5), ("F", 2, 0),
    ("SC", 1, 1), ("G2", 2, 3), ("G1", 2, 2), ("W", 4, 5), ("DA", 2, 0), ("DB", 2, 0), ("GH", 2, 2), ("G3", 2, 3),
    ("N", 2, 3), ("G1", 2, 1), ("F", 2, 3), ("DA", 2, 3), ("G2", 2, 2), ("GH", 2, 1), ("SA", 2, 0), ("SE", 2, 0),
    ("DB", 2, 3), ("G2", 2, 1), ("SA", 2, 3), ("G3", 2, 2), ("N", 2, 2), ("F", 2, 2), ("DA", 2, 2), ("SB", 2, 0),
    ("SE", 2, 3), ("G3", 2, 1), ("N", 2, 1), ("F", 2, 1), ("DA", 2, 1), ("SA", 2, 2), ("DB", 2, 2), ("SB", 2, 3),
    ("DB", 2, 1), ("SC", 2, 0), ("SA", 2, 1), ("SE", 2, 2), ("SB", 2, 2), ("SE", 2, 1), ("SC", 2, 3), ("SB", 2, 1),
    ("SC", 2, 2), ("SC", 2, 1),
)


def layer_kernel(
    tokens, gain_1, gain_2, gain_3, taps_in, fgate, fup, fdown, conv_in, outer_gate, inner_gate, mix_out, sgate, sup, sdown,
    out,
    w, xg, normed, hidden, psend, precv, pown, s1, r1, s2, r2, gi, outer_s, mixed, gains, taps,
    w_load, x_load, w_send, w_recv, y_send, g_recv, s_recv, k_load,
):
    f, t = lax.axis_index("fs"), lax.axis_index("tp")
    z, x = lax.div(f, 4), lax.rem(f, 4)
    y, core = lax.div(t, 2), lax.rem(t, 2)
    other = 1 - core
    zs = [4 * lax.rem(z + i, 4) for i in range(4)]
    xs = [lax.rem(x + i, 4) for i in range(4)]
    ys = [2 * lax.rem(y + i, 4) for i in range(4)]
    slots = [[zs[i] + xs[j] for j in range(4)] for i in range(4)]
    mine, others = [a + core for a in ys], [a + other for a in ys]

    def slot(h, a, b):
        return slots[b][a] if h == 0 else slots[a][b]

    def w_device(h, phase, d):
        return (slot(h, d, 0) if phase == 1 else slot(h, 0, d), t)

    above, below, partner = (f, mine[1]), (f, mine[3]), (f, others[0])

    def load_tokens():
        return pltpu.make_async_copy(tokens, xg.at[0, t], x_load)

    def loads(g):
        sources = []
        if g in (0, 3):
            for s in range(5):
                for a in (fgate, fup) if g == 0 else (sgate, sup):
                    sources.append(a.at[:, pl.ds(128 * s, 128)])
        elif g in (1, 4):
            a = fdown if g == 1 else sdown
            sources = [a.at[pl.ds(128 * s, 128), :] for s in range(5)]
        else:
            sources = [conv_in, outer_gate, inner_gate, mix_out]
        first = GROUPS[g][0]
        return [pltpu.make_async_copy(a, w.at[f, first + i], w_load.at[g]) for i, a in enumerate(sources)]

    def await_bytes(ref, sem):
        pltpu.make_async_copy(ref, ref, sem).wait()

    def load_vectors():
        copies = [pltpu.make_async_copy(a, gains.at[i], k_load.at[i]) for i, a in enumerate((gain_1, gain_2, gain_3))]
        return copies + [pltpu.make_async_copy(taps_in, taps, k_load.at[3])]

    load_tokens().start()
    for g in range(5):
        for copy in loads(g):
            copy.start()
    for copy in load_vectors():
        copy.start()

    barrier = pltpu.get_barrier_semaphore()
    peers = [w_device(h, 1, d) for h in (0, 1) for d in (1, 3)] + [above, below, partner]
    for peer in peers:
        pl.semaphore_signal(barrier, inc=1, device_id=peer, device_id_type=MESH)

    gi[:, pl.ds(0, 8), :] = jnp.zeros((2, 8, 128), F32)

    load_tokens().wait()
    for copy in load_vectors():
        copy.wait()
    pl.semaphore_wait(barrier, len(peers))

    def w_copy(g, h, a, b, phase, d, quarter, landing):
        first, count = GROUPS[g]
        if quarter:
            rows = pl.ds(64 * h + (0 if d == 1 else 32), 32)
        else:
            rows = pl.ds(64 * h, 64)
        part = w.at[slot(h, a, b), pl.ds(first, count), rows]
        pltpu.make_async_remote_copy(
            src_ref=part, dst_ref=part, send_sem=w_send.at[g], recv_sem=w_recv.at[g, landing],
            device_id=w_device(h, phase, d), device_id_type=MESH,
        ).start()

    def w_wait(g, landing):
        first, count = GROUPS[g]
        await_bytes(w.at[pl.ds(0, UNITS[landing]), pl.ds(first, count)], w_recv.at[g, landing])

    both = [(h, d) for h in (0, 1) for d in (1, 3)]

    def weights(g, rnd):
        first, count = GROUPS[g]
        if rnd == 0:
            await_bytes(w.at[f, pl.ds(first, count)], w_load.at[g])
            for h, d in both:
                w_copy(g, h, 0, 0, 1, d, False, 1)
            for h, d in both:
                w_copy(g, h, 0, 0, 2, d, False, 2)
        elif rnd == 5:
            w_wait(g, 5)
            w_wait(g, 6)
        else:
            w_wait(g, rnd)
            for h, d in both:
                back = 4 - d
                if rnd == 1:
                    w_copy(g, h, back, 0, 1, d, True, 2)
                elif rnd == 2:
                    w_copy(g, h, 0, back, 2, d, True, 4)
                elif rnd == 3:
                    w_copy(g, h, 1, back, 2, d, True, 5)
                    w_copy(g, h, 3, back, 2, d, True, 5)
                else:
                    w_copy(g, h, 2, back, 2, d, True, 6)
            for h, d in both:
                if rnd == 1:
                    w_copy(g, h, 1, 0, 2, d, False, 3)
                    w_copy(g, h, 3, 0, 2, d, False, 3)
                elif rnd == 2:
                    w_copy(g, h, 2, 0, 2, d, False, 4)

    def y_copy(src, dst, stage, c, recv, device):
        pltpu.make_async_remote_copy(
            src_ref=src, dst_ref=dst, send_sem=y_send.at[stage, c], recv_sem=recv,
            device_id=device, device_id_type=MESH,
        ).start()

    def rows_of(c):
        return pl.ds(c * R, R)

    def front(c):
        return pl.ds(c * R, HALF)

    def rear(c):
        return pl.ds(c * R + HALF, HALF)

    def gather_0(stage, c):
        ref = xg.at[stage, t, rows_of(c)]
        for landing, parts in ((0, (front(c), rear(c))), (3, (rear(c), front(c)))):
            for part, device in zip(parts, (above, below)):
                half = xg.at[stage, t, part]
                y_copy(half, half, stage, c, g_recv.at[stage, c, landing], device)
        y_copy(ref, ref, stage, c, g_recv.at[stage, c, 2], partner)

    def gather_1(stage, c):
        await_bytes(xg.at[stage, 0, rows_of(c)], g_recv.at[stage, c, 0])
        for block, part, device in ((mine[3], front(c), above), (mine[1], rear(c), below)):
            ref = xg.at[stage, block, part]
            y_copy(ref, ref, stage, c, g_recv.at[stage, c, 1], device)

    def gather_rest(stage, c):
        await_bytes(xg.at[stage, 0, rows_of(c)], g_recv.at[stage, c, 3])
        for block in (mine[3], mine[1]):
            ref = xg.at[stage, block, rows_of(c)]
            y_copy(ref, ref, stage, c, g_recv.at[stage, c, 2], partner)

    def gather_2(stage, c):
        await_bytes(xg.at[stage, 0, rows_of(c)], g_recv.at[stage, c, 1])
        ref = xg.at[stage, mine[2], rows_of(c)]
        y_copy(ref, ref, stage, c, g_recv.at[stage, c, 2], partner)

    def gather_3(stage, c):
        await_bytes(xg.at[stage, pl.ds(0, 4), rows_of(c)], g_recv.at[stage, c, 2])

    def norm(stage, c):
        @pl.loop(0, R // SUB)
        def _(i):
            rows = pl.ds(pl.multiple_of(c * R + i * SUB, SUB), SUB)
            total = jnp.zeros((SUB, BLK), F32)
            for b in range(8):
                v = xg[stage, b, rows, :].astype(F32)
                total = total + v * v
            mean = jnp.sum(total, axis=1, keepdims=True) * (1.0 / D)
            scale = lax.rsqrt(mean + EPS)
            for b in range(8):
                v = xg[stage, b, rows, :].astype(F32)
                cols = pl.ds(b * BLK, BLK)
                normed[rows, cols] = (v * scale * gains[stage, :, cols]).astype(BF16)

    def columns(first):
        return w[:, first].reshape(D, 128)

    def ffn(stage, c):
        first = 0 if stage == 0 else 19

        all_columns = jnp.concatenate([columns(first + 2 * s + i) for i in (0, 1) for s in range(5)], axis=1)
        products = jnp.dot(normed[rows_of(c), :], all_columns, preferred_element_type=F32)
        gate, upward = products[:, :640], products[:, 640:]
        hidden[rows_of(c), :] = (gate / (1.0 + jnp.exp(-gate)) * upward).astype(BF16)

    def mixer(c):
        three = jnp.concatenate([columns(15), columns(16), columns(17)], axis=1)
        products = jnp.dot(normed[rows_of(c), :], three, preferred_element_type=F32)
        seq, at = c * R // LEN, c * R % LEN
        gi[seq, pl.ds(8 + at, R), :] = products[:, 256:] * products[:, :128]
        outer_s[...] = products[:, 128:256]
        convolved = taps[0:1, :] * gi[seq, pl.ds(6 + at, R), :]
        convolved = convolved + taps[1:2, :] * gi[seq, pl.ds(7 + at, R), :]
        convolved = convolved + taps[2:3, :] * gi[seq, pl.ds(8 + at, R), :]
        mixed[rows_of(c), :] = (outer_s[...] * convolved).astype(BF16)

    def product(stage, c, blocks):
        if stage == 1:
            rows, columns = mixed[rows_of(c), :], [w[2 * b + i, 18] for b in blocks for i in (0, 1)]
        else:
            slabs = pl.ds(10 if stage == 0 else 29, 5)
            rows, columns = hidden[rows_of(c), :], [w[2 * b + i, slabs].reshape(640, 128) for b in blocks for i in (0, 1)]
        return jnp.dot(rows, jnp.concatenate(columns, axis=1), preferred_element_type=F32)

    def down(stage, c, first, count, landing):
        products = product(stage, c, [others[AHEAD[i]] for i in range(first, first + count)])
        for i in range(count):
            psend[stage, first + i, rows_of(c), :] = products[:, BLK * i : BLK * (i + 1)].astype(BF16)
        part = pl.ds(first, count)
        y_copy(psend.at[stage, part, rows_of(c)], precv.at[stage, part, rows_of(c)], stage, c, s_recv.at[stage, c, landing], partner)
        products = product(stage, c, [mine[AHEAD[i]] for i in range(first, first + count)])
        for i in range(count):
            pown[first + i, rows_of(c), :] = products[:, BLK * i : BLK * (i + 1)]

    def down_first(stage, c):
        down(stage, c, 0, 1, 0)

    def down_rest(stage, c):
        down(stage, c, 1, 3, 3)

    def pair_sum(stage, i, rows):
        return pown[i, rows, :] + precv[stage, i, rows, :].astype(F32)

    def sum_a(stage, c):
        await_bytes(precv.at[stage, 0, rows_of(c)], s_recv.at[stage, c, 0])
        s1[stage, rows_of(c), :] = pair_sum(stage, 0, rows_of(c)).astype(BF16)
        for part, device in ((front(c), above), (rear(c), below)):
            y_copy(s1.at[stage, part], r1.at[stage, part], stage, c, s_recv.at[stage, c, 1], device)

    def send_halves(stage, c, parts, with_r1):
        for i, part, device in ((1, parts[0], above), (2, parts[1], below)):
            value = pair_sum(stage, i, part)
            if with_r1:
                value = value + r1[stage, part, :].astype(F32)
            s2[stage, i - 1, part, :] = value.astype(BF16)
            y_copy(s2.at[stage, i - 1, part], r2.at[stage, i - 1, part], stage, c, s_recv.at[stage, c, 2], device)

    def sum_early(stage, c):
        await_bytes(precv.at[stage, pl.ds(1, 3), rows_of(c)], s_recv.at[stage, c, 3])
        send_halves(stage, c, (rear(c), front(c)), False)

    def sum_b(stage, c):
        await_bytes(r1.at[stage, rows_of(c)], s_recv.at[stage, c, 1])
        send_halves(stage, c, (front(c), rear(c)), True)

    def sum_c(stage, c):
        await_bytes(r2.at[stage, pl.ds(0, 2), rows_of(c)], s_recv.at[stage, c, 2])

        rows = rows_of(c)
        branch = pair_sum(stage, 3, rows) + r2[stage, 0, rows, :].astype(F32) + r2[stage, 1, rows, :].astype(F32)
        if stage != 1:
            branch = 0.5 * branch
        value = (xg[stage, t, rows, :].astype(F32) + branch).astype(BF16)
        if stage < 2:
            xg[stage + 1, t, rows, :] = value
            gather_0(stage + 1, c)
        else:
            out[rows, :] = value

    def mid(stage, c):
        if stage == 1:
            mixer(c)
        else:
            ffn(stage, c)

    tasks = dict(
        W=weights, G0=gather_0, G1=gather_1, GH=gather_rest, G2=gather_2, G3=gather_3, N=norm, F=mid,
        DA=down_first, DB=down_rest, SA=sum_a, SE=sum_early, SB=sum_b, SC=sum_c,
    )
    for name, a, b in ORDER:
        with jax.named_scope(f"{name}_{a}_{b}"):
            tasks[name](a, b)

    for g, (first, count) in enumerate(GROUPS):
        await_bytes(w.at[pl.ds(0, 15), pl.ds(first, count)], w_send.at[g])
    for stage in range(3):
        for c in range(NC):
            await_bytes(xg.at[0, pl.ds(0, 7), rows_of(c)], y_send.at[stage, c])
            await_bytes(xg.at[0, pl.ds(0, 7), rows_of(c)], y_send.at[stage, c])


def on_device(
    tokens, first_gain, first_gate, first_up, first_down, mixer_gain, conv_input, outer_gate, inner_gate, conv_taps,
    mixer_out, second_gain, second_gate, second_up, second_down,
):
    shape = tokens.shape
    hbm = pl.BlockSpec(memory_space=pl.ANY)
    dma = pltpu.SemaphoreType.DMA
    result = pl.pallas_call(
        layer_kernel,
        out_shape=pltpu.VMEM((ROWS, BLK), BF16),
        in_specs=[hbm] * 15,
        out_specs=pl.BlockSpec(memory_space=pltpu.VMEM),
        scratch_shapes=[
            pltpu.VMEM((16, SLABS, 128, 128), BF16),
            pltpu.VMEM((3, 8, ROWS, BLK), BF16),
            pltpu.VMEM((ROWS, D), BF16),
            pltpu.VMEM((ROWS, 640), BF16),
            pltpu.VMEM((3, 4, ROWS, BLK), BF16),
            pltpu.VMEM((3, 4, ROWS, BLK), BF16),
            pltpu.VMEM((4, ROWS, BLK), F32),
            pltpu.VMEM((3, ROWS, BLK), BF16),
            pltpu.VMEM((3, ROWS, BLK), BF16),
            pltpu.VMEM((3, 2, ROWS, BLK), BF16),
            pltpu.VMEM((3, 2, ROWS, BLK), BF16),
            pltpu.VMEM((2, 8 + LEN, 128), F32),
            pltpu.VMEM((R, 128), F32),
            pltpu.VMEM((ROWS, 128), BF16),
            pltpu.VMEM((3, 1, D), F32),
            pltpu.VMEM((3, 128), F32),
            dma((5,)),
            dma,
            dma((5,)),
            dma((5, 7)),
            dma((3, NC)),
            dma((3, NC, 4)),
            dma((3, NC, 4)),
            dma((4,)),
        ],
        compiler_params=pltpu.CompilerParams(
            collective_id=0, has_side_effects=True, vmem_limit_bytes=60_000_000
        ),
    )(
        tokens.reshape(ROWS, BLK), first_gain[None], mixer_gain[None], second_gain[None], conv_taps, first_gate, first_up, first_down, conv_input, outer_gate,
        inner_gate, mixer_out, second_gate, second_up, second_down,
    )
    return result.reshape(shape)


def solution(mesh):
    fs, tp = P("fs", "tp"), P("tp", "fs")
    in_specs = (
        P("fs", None, "tp"), P(), fs, fs, tp, P(), fs, fs, fs, P(None, "tp"), tp, P(), fs, fs, tp,
    )
    return jax.shard_map(
        on_device, mesh=mesh, in_specs=in_specs, out_specs=P("fs", None, "tp"), check_vma=False
    )
```

```python
import functools

import jax
import jax.numpy as jnp
from jax import lax
from jax.experimental import pallas as pl
from jax.experimental.pallas import tpu as pltpu
from jax.sharding import PartitionSpec as P

EPS = 1e-05
MESH = pl.DeviceIdType.MESH
F32, BF16 = jnp.float32, jnp.bfloat16

D = 2048
ROWS = 768
LEN = 384
BLK = 256
NC = 4
R = ROWS // NC
HALF = R // 2
SUB = 96
SLABS = 34
GROUPS = ((0, 10), (10, 5), (15, 4), (19, 10), (29, 5))
UNITS = (0, 2, 3, 4, 3, 2, 1)
AHEAD = (2, 1, 3, 0)


ORDER = (
    ("W", 0, 0), ("G0", 0, 2), ("G0", 0, 3), ("G1", 0, 2), ("G0", 0, 0), ("W", 0, 1), ("G1", 0, 0), ("GH", 0, 0),
    ("G1", 0, 3), ("W", 1, 0), ("W", 0, 2), ("G0", 0, 1), ("W", 0, 3), ("G1", 0, 1), ("GH", 0, 1), ("W", 1, 1),
    ("GH", 0, 2), ("G2", 0, 2), ("G3", 0, 2), ("G2", 0, 1), ("GH", 0, 3), ("G2", 0, 0), ("N", 0, 2), ("G2", 0, 3),
    ("G3", 0, 3), ("N", 0, 3), ("G3", 0, 0), ("N", 0, 0), ("W", 1, 2), ("W", 0, 4), ("G3", 0, 1), ("W", 1, 3),
    ("N", 0, 1), ("W", 1, 4), ("W", 2, 0), ("W", 3, 0), ("W", 0, 5), ("F", 0, 3), ("F", 0, 0), ("W", 1, 5),
    ("DA", 0, 0), ("DA", 0, 3), ("DB", 0, 3), ("DB", 0, 0), ("SA", 0, 0), ("SA", 0, 3), ("F", 0, 2), ("DA", 0, 2),
    ("SE", 0, 0), ("DB", 0, 2), ("W", 2, 1), ("SB", 0, 0), ("SE", 0, 3), ("SA", 0, 2), ("F", 0, 1), ("SE", 0, 2),
    ("W", 2, 2), ("SC", 0, 0), ("DA", 0, 1), ("SB", 0, 2), ("SB", 0, 3), ("W", 4, 0), ("G1", 1, 0), ("DB", 0, 1),
    ("W", 2, 3), ("SA", 0, 1), ("W", 2, 4), ("SC", 0, 2), ("W", 3, 1), ("SC", 0, 3), ("GH", 1, 0), ("G2", 1, 0),
    ("G1", 1, 2), ("SE", 0, 1), ("W", 2, 5), ("SB", 0, 1), ("G3", 1, 0), ("N", 1, 0), ("W", 4, 1), ("GH", 1, 2),
    ("F", 1, 0), ("DA", 1, 0), ("DB", 1, 0), ("G1", 1, 3), ("G2", 1, 2), ("SA", 1, 0), ("SC", 0, 1), ("GH", 1, 3),
    ("G2", 1, 3), ("G3", 1, 2), ("N", 1, 2), ("F", 1, 2), ("SE", 1, 0), ("DA", 1, 2), ("SB", 1, 0), ("DB", 1, 2),
    ("W", 3, 2), ("G3", 1, 3), ("N", 1, 3), ("G1", 1, 1), ("F", 1, 3), ("DA", 1, 3), ("W", 3, 3), ("SA", 1, 2),
    ("SE", 1, 2), ("DB", 1, 3), ("GH", 1, 1), ("SA", 1, 3), ("G2", 1, 1), ("SC", 1, 0), ("SE", 1, 3), ("W", 4, 2),
    ("G3", 1, 1), ("N", 1, 1), ("F", 1, 1), ("SB", 1, 3), ("DA", 1, 1), ("SB", 1, 2), ("G1", 2, 0), ("GH", 2, 0),
    ("DB", 1, 1), ("W", 3, 4), ("W", 4, 3), ("SA", 1, 1), ("SC", 1, 3), ("G2", 2, 0), ("SE", 1, 1), ("SB", 1, 1),
    ("W", 4, 4), ("G1", 2, 3), ("GH", 2, 3), ("G3", 2, 0), ("SC", 1, 2), ("N", 2, 0), ("W", 3, 5), ("F", 2, 0),
    ("SC", 1, 1), ("G2", 2, 3), ("G1", 2, 2), ("W", 4, 5), ("DA", 2, 0), ("DB", 2, 0), ("GH", 2, 2), ("G3", 2, 3),
    ("N", 2, 3), ("G1", 2, 1), ("F", 2, 3), ("DA", 2, 3), ("G2", 2, 2), ("GH", 2, 1), ("SA", 2, 0), ("SE", 2, 0),
    ("DB", 2, 3), ("G2", 2, 1), ("SA", 2, 3), ("G3", 2, 2), ("N", 2, 2), ("F", 2, 2), ("DA", 2, 2), ("SB", 2, 0),
    ("SE", 2, 3), ("G3", 2, 1), ("N", 2, 1), ("F", 2, 1), ("DA", 2, 1), ("SA", 2, 2), ("DB", 2, 2), ("SB", 2, 3),
    ("DB", 2, 1), ("SC", 2, 0), ("SA", 2, 1), ("SE", 2, 2), ("SB", 2, 2), ("SE", 2, 1), ("SC", 2, 3), ("SB", 2, 1),
    ("SC", 2, 2), ("SC", 2, 1),
)


def layer_kernel(
    tokens, gain_1, gain_2, gain_3, taps_in, fgate, fup, fdown, conv_in, outer_gate, inner_gate, mix_out, sgate, sup, sdown,
    out,
    w, xg, normed, hidden, psend, precv, pown, s1, r1, s2, r2, gi, outer_s, mixed, gains, taps,
    w_load, x_load, w_send, w_recv, y_send, g_recv, s_recv, k_load,
):
    f, t = lax.axis_index("fs"), lax.axis_index("tp")
    z, x = lax.div(f, 4), lax.rem(f, 4)
    y, core = lax.div(t, 2), lax.rem(t, 2)
    other = 1 - core
    zs = [4 * lax.rem(z + i, 4) for i in range(4)]
    xs = [lax.rem(x + i, 4) for i in range(4)]
    ys = [2 * lax.rem(y + i, 4) for i in range(4)]
    slots = [[zs[i] + xs[j] for j in range(4)] for i in range(4)]
    mine, others = [a + core for a in ys], [a + other for a in ys]

    def slot(h, a, b):
        return slots[b][a] if h == 0 else slots[a][b]

    def w_device(h, phase, d):
        return (slot(h, d, 0) if phase == 1 else slot(h, 0, d), t)

    above, below, partner = (f, mine[1]), (f, mine[3]), (f, others[0])

    def load_tokens():
        return pltpu.make_async_copy(tokens, xg.at[0, t], x_load)

    def loads(g):
        sources = []
        if g in (0, 3):
            for s in range(5):
                for a in (fgate, fup) if g == 0 else (sgate, sup):
                    sources.append(a.at[:, pl.ds(128 * s, 128)])
        elif g in (1, 4):
            a = fdown if g == 1 else sdown
            sources = [a.at[pl.ds(128 * s, 128), :] for s in range(5)]
        else:
            sources = [conv_in, outer_gate, inner_gate, mix_out]
        first = GROUPS[g][0]
        return [pltpu.make_async_copy(a, w.at[f, first + i], w_load.at[g]) for i, a in enumerate(sources)]

    def await_bytes(ref, sem):
        pltpu.make_async_copy(ref, ref, sem).wait()

    def load_vectors():
        copies = [pltpu.make_async_copy(a, gains.at[i], k_load.at[i]) for i, a in enumerate((gain_1, gain_2, gain_3))]
        return copies + [pltpu.make_async_copy(taps_in, taps, k_load.at[3])]

    load_tokens().start()
    for g in range(5):
        for copy in loads(g):
            copy.start()
    for copy in load_vectors():
        copy.start()

    barrier = pltpu.get_barrier_semaphore()
    peers = [w_device(h, 1, d) for h in (0, 1) for d in (1, 3)] + [above, below, partner]
    for peer in peers:
        pl.semaphore_signal(barrier, inc=1, device_id=peer, device_id_type=MESH)

    gi[:, pl.ds(0, 8), :] = jnp.zeros((2, 8, 128), F32)

    load_tokens().wait()
    for copy in load_vectors():
        copy.wait()
    pl.semaphore_wait(barrier, len(peers))

    def w_copy(g, h, a, b, phase, d, quarter, landing):
        first, count = GROUPS[g]
        if quarter:
            rows = pl.ds(64 * h + (0 if d == 1 else 32), 32)
        else:
            rows = pl.ds(64 * h, 64)
        part = w.at[slot(h, a, b), pl.ds(first, count), rows]
        pltpu.make_async_remote_copy(
            src_ref=part, dst_ref=part, send_sem=w_send.at[g], recv_sem=w_recv.at[g, landing - 1],
            device_id=w_device(h, phase, d), device_id_type=MESH,
        ).start()

    def w_wait(g, landing):
        first, count = GROUPS[g]
        await_bytes(w.at[pl.ds(0, UNITS[landing]), pl.ds(first, count)], w_recv.at[g, landing - 1])

    both = [(h, d) for h in (0, 1) for d in (1, 3)]

    def weights(g, rnd):
        first, count = GROUPS[g]
        if rnd == 0:
            await_bytes(w.at[f, pl.ds(first, count)], w_load.at[g])
            for h, d in both:
                w_copy(g, h, 0, 0, 1, d, False, 1)
            for h, d in both:
                w_copy(g, h, 0, 0, 2, d, False, 2)
        elif rnd == 5:
            w_wait(g, 5)
            w_wait(g, 6)
        else:
            w_wait(g, rnd)
            for h, d in both:
                back = 4 - d
                if rnd == 1:
                    w_copy(g, h, back, 0, 1, d, True, 2)
                elif rnd == 2:
                    w_copy(g, h, 0, back, 2, d, True, 4)
                elif rnd == 3:
                    w_copy(g, h, 1, back, 2, d, True, 5)
                    w_copy(g, h, 3, back, 2, d, True, 5)
                else:
                    w_copy(g, h, 2, back, 2, d, True, 6)
            for h, d in both:
                if rnd == 1:
                    w_copy(g, h, 1, 0, 2, d, False, 3)
                    w_copy(g, h, 3, 0, 2, d, False, 3)
                elif rnd == 2:
                    w_copy(g, h, 2, 0, 2, d, False, 4)

    def y_copy(src, dst, stage, c, recv, device):
        pltpu.make_async_remote_copy(
            src_ref=src, dst_ref=dst, send_sem=y_send.at[stage], recv_sem=recv,
            device_id=device, device_id_type=MESH,
        ).start()

    def rows_of(c):
        return pl.ds(c * R, R)

    def front(c):
        return pl.ds(c * R, HALF)

    def rear(c):
        return pl.ds(c * R + HALF, HALF)

    def gather_0(stage, c):
        ref = xg.at[stage, t, rows_of(c)]
        for landing, parts in ((0, (front(c), rear(c))), (3, (rear(c), front(c)))):
            for part, device in zip(parts, (above, below)):
                half = xg.at[stage, t, part]
                y_copy(half, half, stage, c, g_recv.at[c, landing], device)
        y_copy(ref, ref, stage, c, g_recv.at[c, 2], partner)

    def gather_1(stage, c):
        await_bytes(xg.at[stage, 0, rows_of(c)], g_recv.at[c, 0])
        for block, part, device in ((mine[3], front(c), above), (mine[1], rear(c), below)):
            ref = xg.at[stage, block, part]
            y_copy(ref, ref, stage, c, g_recv.at[c, 1], device)

    def gather_rest(stage, c):
        await_bytes(xg.at[stage, 0, rows_of(c)], g_recv.at[c, 3])
        for block in (mine[3], mine[1]):
            ref = xg.at[stage, block, rows_of(c)]
            y_copy(ref, ref, stage, c, g_recv.at[c, 2], partner)

    def gather_2(stage, c):
        await_bytes(xg.at[stage, 0, rows_of(c)], g_recv.at[c, 1])
        ref = xg.at[stage, mine[2], rows_of(c)]
        y_copy(ref, ref, stage, c, g_recv.at[c, 2], partner)

    def gather_3(stage, c):
        await_bytes(xg.at[stage, pl.ds(0, 4), rows_of(c)], g_recv.at[c, 2])

    def norm(stage, c):
        @pl.loop(0, R // SUB)
        def _(i):
            rows = pl.ds(pl.multiple_of(c * R + i * SUB, SUB), SUB)
            total = jnp.zeros((SUB, BLK), F32)
            for b in range(8):
                v = xg[stage, b, rows, :].astype(F32)
                total = total + v * v
            mean = jnp.sum(total, axis=1, keepdims=True) * (1.0 / D)
            scale = lax.rsqrt(mean + EPS)
            for b in range(8):
                v = xg[stage, b, rows, :].astype(F32)
                cols = pl.ds(b * BLK, BLK)
                normed[rows, cols] = (v * scale * gains[stage, :, cols]).astype(BF16)

    def columns(first):
        return w[:, first].reshape(D, 128)

    def ffn(stage, c):
        first = 0 if stage == 0 else 19

        all_columns = jnp.concatenate([columns(first + 2 * s + i) for i in (0, 1) for s in range(5)], axis=1)
        products = jnp.dot(normed[rows_of(c), :], all_columns, preferred_element_type=F32)
        gate, upward = products[:, :640], products[:, 640:]
        hidden[rows_of(c), :] = (gate / (1.0 + jnp.exp(-gate)) * upward).astype(BF16)

    def mixer(c):
        three = jnp.concatenate([columns(15), columns(16), columns(17)], axis=1)
        products = jnp.dot(normed[rows_of(c), :], three, preferred_element_type=F32)
        seq, at = c * R // LEN, c * R % LEN
        gi[seq, pl.ds(8 + at, R), :] = products[:, 256:] * products[:, :128]
        outer_s[...] = products[:, 128:256]
        convolved = taps[0:1, :] * gi[seq, pl.ds(6 + at, R), :]
        convolved = convolved + taps[1:2, :] * gi[seq, pl.ds(7 + at, R), :]
        convolved = convolved + taps[2:3, :] * gi[seq, pl.ds(8 + at, R), :]
        mixed[rows_of(c), :] = (outer_s[...] * convolved).astype(BF16)

    def product(stage, c, blocks):
        if stage == 1:
            rows, columns = mixed[rows_of(c), :], [w[2 * b + i, 18] for b in blocks for i in (0, 1)]
        else:
            slabs = pl.ds(10 if stage == 0 else 29, 5)
            rows, columns = hidden[rows_of(c), :], [w[2 * b + i, slabs].reshape(640, 128) for b in blocks for i in (0, 1)]
        return jnp.dot(rows, jnp.concatenate(columns, axis=1), preferred_element_type=F32)

    def down(stage, c, first, count, landing):
        ahead = AHEAD[first : first + count]
        products = product(stage, c, [others[i] for i in ahead] + [mine[i] for i in ahead])
        for i in range(count):
            psend[stage, first + i, rows_of(c), :] = products[:, BLK * i : BLK * (i + 1)].astype(BF16)
        part = pl.ds(first, count)
        y_copy(psend.at[stage, part, rows_of(c)], precv.at[stage, part, rows_of(c)], stage, c, s_recv.at[c, landing], partner)
        for i in range(count):
            pown[first + i, rows_of(c), :] = products[:, BLK * (count + i) : BLK * (count + i + 1)]

    def down_first(stage, c):
        down(stage, c, 0, 1, 0)

    def down_rest(stage, c):
        down(stage, c, 1, 3, 3)

    def pair_sum(stage, i, rows):
        return pown[i, rows, :] + precv[stage, i, rows, :].astype(F32)

    def sum_a(stage, c):
        await_bytes(precv.at[stage, 0, rows_of(c)], s_recv.at[c, 0])
        s1[stage, rows_of(c), :] = pair_sum(stage, 0, rows_of(c)).astype(BF16)
        for part, device in ((front(c), above), (rear(c), below)):
            y_copy(s1.at[stage, part], r1.at[stage, part], stage, c, s_recv.at[c, 1], device)

    def send_halves(stage, c, parts, with_r1):
        for i, part, device in ((1, parts[0], above), (2, parts[1], below)):
            value = pair_sum(stage, i, part)
            if with_r1:
                value = value + r1[stage, part, :].astype(F32)
            s2[stage, i - 1, part, :] = value.astype(BF16)
            y_copy(s2.at[stage, i - 1, part], r2.at[stage, i - 1, part], stage, c, s_recv.at[c, 2], device)

    def sum_early(stage, c):
        await_bytes(precv.at[stage, pl.ds(1, 3), rows_of(c)], s_recv.at[c, 3])
        send_halves(stage, c, (rear(c), front(c)), False)

    def sum_b(stage, c):
        await_bytes(r1.at[stage, rows_of(c)], s_recv.at[c, 1])
        send_halves(stage, c, (front(c), rear(c)), True)

    def sum_c(stage, c):
        await_bytes(r2.at[stage, pl.ds(0, 2), rows_of(c)], s_recv.at[c, 2])

        rows = rows_of(c)
        branch = pair_sum(stage, 3, rows) + r2[stage, 0, rows, :].astype(F32) + r2[stage, 1, rows, :].astype(F32)
        if stage != 1:
            branch = 0.5 * branch
        value = (xg[stage, t, rows, :].astype(F32) + branch).astype(BF16)
        if stage < 2:
            xg[stage + 1, t, rows, :] = value
            gather_0(stage + 1, c)
        else:
            out[rows, :] = value

    def mid(stage, c):
        if stage == 1:
            mixer(c)
        else:
            ffn(stage, c)

    tasks = dict(
        W=weights, G0=gather_0, G1=gather_1, GH=gather_rest, G2=gather_2, G3=gather_3, N=norm, F=mid,
        DA=down_first, DB=down_rest, SA=sum_a, SE=sum_early, SB=sum_b, SC=sum_c,
    )

    def sent(stage):
        for _ in range(2):
            await_bytes(xg.at[0, pl.ds(0, 7)], y_send.at[stage])

    for step, (name, a, b) in enumerate(ORDER):
        if step == len(ORDER) - 2:
            for g, (first, count) in enumerate(GROUPS):
                await_bytes(w.at[pl.ds(0, 15), pl.ds(first, count)], w_send.at[g])
            sent(0)
            sent(1)
        with jax.named_scope(f"{name}_{a}_{b}"):
            tasks[name](a, b)

    sent(2)


def on_device(
    tokens, first_gain, first_gate, first_up, first_down, mixer_gain, conv_input, outer_gate, inner_gate, conv_taps,
    mixer_out, second_gain, second_gate, second_up, second_down,
):
    shape = tokens.shape
    hbm = pl.BlockSpec(memory_space=pl.ANY)
    dma = pltpu.SemaphoreType.DMA
    result = pl.pallas_call(
        layer_kernel,
        out_shape=pltpu.VMEM((ROWS, BLK), BF16),
        in_specs=[hbm] * 15,
        out_specs=pl.BlockSpec(memory_space=pltpu.VMEM),
        scratch_shapes=[
            pltpu.VMEM((16, SLABS, 128, 128), BF16),
            pltpu.VMEM((3, 8, ROWS, BLK), BF16),
            pltpu.VMEM((ROWS, D), BF16),
            pltpu.VMEM((ROWS, 640), BF16),
            pltpu.VMEM((3, 4, ROWS, BLK), BF16),
            pltpu.VMEM((3, 4, ROWS, BLK), BF16),
            pltpu.VMEM((4, ROWS, BLK), F32),
            pltpu.VMEM((3, ROWS, BLK), BF16),
            pltpu.VMEM((3, ROWS, BLK), BF16),
            pltpu.VMEM((3, 2, ROWS, BLK), BF16),
            pltpu.VMEM((3, 2, ROWS, BLK), BF16),
            pltpu.VMEM((2, 8 + LEN, 128), F32),
            pltpu.VMEM((R, 128), F32),
            pltpu.VMEM((ROWS, 128), BF16),
            pltpu.VMEM((3, 1, D), F32),
            pltpu.VMEM((3, 128), F32),
            dma((5,)),
            dma,
            dma((5,)),
            dma((5, 6)),
            dma((3,)),
            dma((NC, 4)),
            dma((NC, 4)),
            dma((4,)),
        ],
        compiler_params=pltpu.CompilerParams(
            collective_id=0, has_side_effects=True, vmem_limit_bytes=60_000_000
        ),
    )(
        tokens.reshape(ROWS, BLK), first_gain[None], mixer_gain[None], second_gain[None], conv_taps, first_gate, first_up, first_down, conv_input, outer_gate,
        inner_gate, mixer_out, second_gate, second_up, second_down,
    )
    return result.reshape(shape)


def solution(mesh):
    fs, tp = P("fs", "tp"), P("tp", "fs")
    in_specs = (
        P("fs", None, "tp"), P(), fs, fs, tp, P(), fs, fs, fs, P(None, "tp"), tp, P(), fs, fs, tp,
    )
    return jax.shard_map(
        on_device, mesh=mesh, in_specs=in_specs, out_specs=P("fs", None, "tp"), check_vma=False
    )
```

```python
import functools

import jax
import jax.numpy as jnp
from jax import lax
from jax.experimental import pallas as pl
from jax.experimental.pallas import tpu as pltpu
from jax.sharding import PartitionSpec as P

EPS = 1e-05
MESH = pl.DeviceIdType.MESH
F32, BF16 = jnp.float32, jnp.bfloat16

D = 2048
ROWS = 768
LEN = 384
BLK = 256
NC = 4
R = ROWS // NC
HALF = R // 2
SUB = 96
SLABS = 34
GROUPS = ((0, 10), (10, 5), (15, 4), (19, 10), (29, 5))
UNITS = (0, 2, 3, 4, 2, 4)
AHEAD = (2, 1, 3, 0)


ORDER = (
    ("W", 0, 0), ("G0", 0, 2), ("G0", 0, 3), ("G1", 0, 2), ("G0", 0, 0), ("W", 0, 1), ("G1", 0, 0), ("GH", 0, 0),
    ("G1", 0, 3), ("W", 1, 0), ("W", 0, 2), ("G0", 0, 1), ("W", 0, 3), ("G1", 0, 1), ("GH", 0, 1), ("W", 1, 1),
    ("GH", 0, 2), ("G2", 0, 2), ("G3", 0, 2), ("G2", 0, 1), ("GH", 0, 3), ("G2", 0, 0), ("N", 0, 2), ("G2", 0, 3),
    ("G3", 0, 3), ("N", 0, 3), ("G3", 0, 0), ("N", 0, 0), ("W", 1, 2), ("W", 0, 4), ("G3", 0, 1), ("W", 1, 3),
    ("N", 0, 1), ("W", 1, 4), ("W", 2, 0), ("W", 3, 0), ("W", 0, 5), ("F", 0, 3), ("F", 0, 0), ("W", 1, 5),
    ("DA", 0, 0), ("DA", 0, 3), ("DB", 0, 3), ("DB", 0, 0), ("SA", 0, 0), ("SA", 0, 3), ("F", 0, 2), ("DA", 0, 2),
    ("SE", 0, 0), ("DB", 0, 2), ("W", 2, 1), ("SB", 0, 0), ("SE", 0, 3), ("SA", 0, 2), ("F", 0, 1), ("SE", 0, 2),
    ("W", 2, 2), ("SC", 0, 0), ("DA", 0, 1), ("SB", 0, 2), ("SB", 0, 3), ("W", 4, 0), ("G1", 1, 0), ("DB", 0, 1),
    ("W", 2, 3), ("SA", 0, 1), ("W", 2, 4), ("SC", 0, 2), ("W", 3, 1), ("SC", 0, 3), ("GH", 1, 0), ("G2", 1, 0),
    ("G1", 1, 2), ("SE", 0, 1), ("W", 2, 5), ("SB", 0, 1), ("G3", 1, 0), ("N", 1, 0), ("W", 4, 1), ("GH", 1, 2),
    ("F", 1, 0), ("DA", 1, 0), ("DB", 1, 0), ("G1", 1, 3), ("G2", 1, 2), ("SA", 1, 0), ("SC", 0, 1), ("GH", 1, 3),
    ("G2", 1, 3), ("G3", 1, 2), ("N", 1, 2), ("F", 1, 2), ("SE", 1, 0), ("DA", 1, 2), ("SB", 1, 0), ("DB", 1, 2),
    ("W", 3, 2), ("G3", 1, 3), ("N", 1, 3), ("G1", 1, 1), ("F", 1, 3), ("DA", 1, 3), ("W", 3, 3), ("SA", 1, 2),
    ("SE", 1, 2), ("DB", 1, 3), ("GH", 1, 1), ("SA", 1, 3), ("G2", 1, 1), ("SC", 1, 0), ("SE", 1, 3), ("W", 4, 2),
    ("G3", 1, 1), ("N", 1, 1), ("F", 1, 1), ("SB", 1, 3), ("DA", 1, 1), ("SB", 1, 2), ("G1", 2, 0), ("GH", 2, 0),
    ("DB", 1, 1), ("W", 3, 4), ("W", 4, 3), ("SA", 1, 1), ("SC", 1, 3), ("G2", 2, 0), ("SE", 1, 1), ("SB", 1, 1),
    ("W", 4, 4), ("G1", 2, 3), ("GH", 2, 3), ("G3", 2, 0), ("SC", 1, 2), ("N", 2, 0), ("W", 3, 5), ("F", 2, 0),
    ("SC", 1, 1), ("G2", 2, 3), ("G1", 2, 2), ("W", 4, 5), ("DA", 2, 0), ("DB", 2, 0), ("GH", 2, 2), ("G3", 2, 3),
    ("N", 2, 3), ("G1", 2, 1), ("F", 2, 3), ("DA", 2, 3), ("G2", 2, 2), ("GH", 2, 1), ("SA", 2, 0), ("SE", 2, 0),
    ("DB", 2, 3), ("G2", 2, 1), ("SA", 2, 3), ("G3", 2, 2), ("N", 2, 2), ("F", 2, 2), ("DA", 2, 2), ("SB", 2, 0),
    ("SE", 2, 3), ("G3", 2, 1), ("N", 2, 1), ("F", 2, 1), ("DA", 2, 1), ("SA", 2, 2), ("DB", 2, 2), ("SB", 2, 3),
    ("DB", 2, 1), ("SC", 2, 0), ("SA", 2, 1), ("SE", 2, 2), ("SB", 2, 2), ("SE", 2, 1), ("SC", 2, 3), ("SB", 2, 1),
    ("SC", 2, 2), ("SC", 2, 1),
)


def layer_kernel(
    tokens, gain_1, gain_2, gain_3, taps_in, fgate, fup, fdown, conv_in, outer_gate, inner_gate, mix_out, sgate, sup, sdown,
    out,
    w, xg, normed, hidden, psend, precv, pown, s1, r1, s2, r2, gi, outer_s, mixed, gains, taps,
    w_load, x_load, w_send, w_recv, y_send, g_recv, s_recv, k_load,
):
    f, t = lax.axis_index("fs"), lax.axis_index("tp")
    z, x = lax.div(f, 4), lax.rem(f, 4)
    y, core = lax.div(t, 2), lax.rem(t, 2)
    other = 1 - core
    zs = [4 * lax.rem(z + i, 4) for i in range(4)]
    xs = [lax.rem(x + i, 4) for i in range(4)]
    ys = [2 * lax.rem(y + i, 4) for i in range(4)]
    slots = [[zs[i] + xs[j] for j in range(4)] for i in range(4)]
    mine, others = [a + core for a in ys], [a + other for a in ys]

    def slot(h, a, b):
        return slots[b][a] if h == 0 else slots[a][b]

    def w_device(h, phase, d):
        return (slot(h, d, 0) if phase == 1 else slot(h, 0, d), t)

    above, below, partner = (f, mine[1]), (f, mine[3]), (f, others[0])

    def load_tokens():
        return pltpu.make_async_copy(tokens, xg.at[0, t], x_load)

    def loads(g):
        sources = []
        if g in (0, 3):
            for s in range(5):
                for a in (fgate, fup) if g == 0 else (sgate, sup):
                    sources.append(a.at[:, pl.ds(128 * s, 128)])
        elif g in (1, 4):
            a = fdown if g == 1 else sdown
            sources = [a.at[pl.ds(128 * s, 128), :] for s in range(5)]
        else:
            sources = [conv_in, outer_gate, inner_gate, mix_out]
        first = GROUPS[g][0]
        return [pltpu.make_async_copy(a, w.at[f, first + i], w_load.at[min(g, 1)]) for i, a in enumerate(sources)]

    def await_bytes(ref, sem):
        pltpu.make_async_copy(ref, ref, sem).wait()

    def load_vectors():
        copies = [pltpu.make_async_copy(a, gains.at[i], k_load.at[0]) for i, a in enumerate((gain_1, gain_2, gain_3))]
        return copies + [pltpu.make_async_copy(taps_in, taps, k_load.at[1])]

    load_tokens().start()
    for g in range(5):
        for copy in loads(g):
            copy.start()
    for copy in load_vectors():
        copy.start()

    barrier = pltpu.get_barrier_semaphore()
    peers = [w_device(h, 1, d) for h in (0, 1) for d in (1, 3)] + [above, below, partner]
    for peer in peers:
        pl.semaphore_signal(barrier, inc=1, device_id=peer, device_id_type=MESH)

    gi[:, pl.ds(0, 8), :] = jnp.zeros((2, 8, 128), F32)

    load_tokens().wait()
    await_bytes(gains, k_load.at[0])
    await_bytes(taps, k_load.at[1])
    pl.semaphore_wait(barrier, len(peers))

    def w_copy(g, h, a, b, phase, d, quarter, landing):
        first, count = GROUPS[g]
        if quarter:
            rows = pl.ds(64 * h + (0 if (d == 1) == (quarter == 1) else 32), 32)
        else:
            rows = pl.ds(64 * h, 64)
        part = w.at[slot(h, a, b), pl.ds(first, count), rows]
        pltpu.make_async_remote_copy(
            src_ref=part, dst_ref=part, send_sem=w_send.at[g], recv_sem=w_recv.at[g, landing - 1],
            device_id=w_device(h, phase, d), device_id_type=MESH,
        ).start()

    def w_wait(g, landing):
        first, count = GROUPS[g]
        await_bytes(w.at[pl.ds(0, UNITS[landing]), pl.ds(first, count)], w_recv.at[g, landing - 1])

    both = [(h, d) for h in (0, 1) for d in (1, 3)]

    def weights(g, rnd):
        first, count = GROUPS[g]
        if rnd == 0:
            if g < 2:
                loaded = pl.ds(0, 10) if g == 0 else pl.ds(10, SLABS - 10)
                await_bytes(w.at[f, loaded], w_load.at[g])
            for h, d in both:
                w_copy(g, h, 0, 0, 1, d, 0, 1)
            for h, d in both:
                w_copy(g, h, 0, 0, 2, d, 0, 2)
        elif rnd == 5:
            w_wait(g, 5)
        else:
            w_wait(g, rnd)
            for h, d in both:
                back = 4 - d
                if rnd == 1:
                    w_copy(g, h, back, 0, 1, d, 1, 2)
                elif rnd == 2:
                    w_copy(g, h, 0, back, 2, d, 1, 4)
                    w_copy(g, h, 2, 0, 2, d, 1, 4)
                elif rnd == 3:
                    w_copy(g, h, 1, back, 2, d, 1, 5)
                    w_copy(g, h, 3, back, 2, d, 1, 5)
                else:
                    w_copy(g, h, 2, back, 2, d, 1, 5)
            for h, d in both:
                if rnd == 1:
                    w_copy(g, h, 1, 0, 2, d, 0, 3)
                    w_copy(g, h, 3, 0, 2, d, 0, 3)
                elif rnd == 2:
                    w_copy(g, h, 2, 0, 2, d, 2, 5)

    def y_copy(src, dst, stage, c, recv, device):
        pltpu.make_async_remote_copy(
            src_ref=src, dst_ref=dst, send_sem=y_send.at[stage], recv_sem=recv,
            device_id=device, device_id_type=MESH,
        ).start()

    def rows_of(c):
        return pl.ds(c * R, R)

    def front(c):
        return pl.ds(c * R, HALF)

    def rear(c):
        return pl.ds(c * R + HALF, HALF)

    def gather_0(stage, c):
        ref = xg.at[stage, t, rows_of(c)]
        for landing, parts in ((0, (front(c), rear(c))), (3, (rear(c), front(c)))):
            for part, device in zip(parts, (above, below)):
                half = xg.at[stage, t, part]
                y_copy(half, half, stage, c, g_recv.at[c, landing], device)
        y_copy(ref, ref, stage, c, g_recv.at[c, 2], partner)

    def gather_1(stage, c):
        await_bytes(xg.at[stage, 0, rows_of(c)], g_recv.at[c, 0])
        for block, part, device in ((mine[3], front(c), above), (mine[1], rear(c), below)):
            ref = xg.at[stage, block, part]
            y_copy(ref, ref, stage, c, g_recv.at[c, 1], device)

    def gather_rest(stage, c):
        await_bytes(xg.at[stage, 0, rows_of(c)], g_recv.at[c, 3])
        for block in (mine[3], mine[1]):
            ref = xg.at[stage, block, rows_of(c)]
            y_copy(ref, ref, stage, c, g_recv.at[c, 2], partner)

    def gather_2(stage, c):
        await_bytes(xg.at[stage, 0, rows_of(c)], g_recv.at[c, 1])
        ref = xg.at[stage, mine[2], rows_of(c)]
        y_copy(ref, ref, stage, c, g_recv.at[c, 2], partner)

    def gather_3(stage, c):
        await_bytes(xg.at[stage, pl.ds(0, 4), rows_of(c)], g_recv.at[c, 2])

    def norm(stage, c):
        @pl.loop(0, R // SUB)
        def _(i):
            rows = pl.ds(pl.multiple_of(c * R + i * SUB, SUB), SUB)
            total = jnp.zeros((SUB, BLK), F32)
            for b in range(8):
                v = xg[stage, b, rows, :].astype(F32)
                total = total + v * v
            mean = jnp.sum(total, axis=1, keepdims=True) * (1.0 / D)
            scale = lax.rsqrt(mean + EPS)
            for b in range(8):
                v = xg[stage, b, rows, :].astype(F32)
                cols = pl.ds(b * BLK, BLK)
                normed[rows, cols] = (v * scale * gains[stage, :, cols]).astype(BF16)

    def columns(first):
        return w[:, first].reshape(D, 128)

    def ffn(stage, c):
        first = 0 if stage == 0 else 19

        all_columns = jnp.concatenate([columns(first + 2 * s + i) for i in (0, 1) for s in range(5)], axis=1)
        products = jnp.dot(normed[rows_of(c), :], all_columns, preferred_element_type=F32)
        gate, upward = products[:, :640], products[:, 640:]
        hidden[rows_of(c), :] = (gate / (1.0 + jnp.exp(-gate)) * upward).astype(BF16)

    def mixer(c):
        three = jnp.concatenate([columns(15), columns(16), columns(17)], axis=1)
        products = jnp.dot(normed[rows_of(c), :], three, preferred_element_type=F32)
        seq, at = c * R // LEN, c * R % LEN
        gi[seq, pl.ds(8 + at, R), :] = products[:, 256:] * products[:, :128]
        outer_s[...] = products[:, 128:256]
        convolved = taps[0:1, :] * gi[seq, pl.ds(6 + at, R), :]
        convolved = convolved + taps[1:2, :] * gi[seq, pl.ds(7 + at, R), :]
        convolved = convolved + taps[2:3, :] * gi[seq, pl.ds(8 + at, R), :]
        mixed[rows_of(c), :] = (outer_s[...] * convolved).astype(BF16)

    def product(stage, c, blocks):
        if stage == 1:
            rows, columns = mixed[rows_of(c), :], [w[2 * b + i, 18] for b in blocks for i in (0, 1)]
        else:
            slabs = pl.ds(10 if stage == 0 else 29, 5)
            rows, columns = hidden[rows_of(c), :], [w[2 * b + i, slabs].reshape(640, 128) for b in blocks for i in (0, 1)]
        return jnp.dot(rows, jnp.concatenate(columns, axis=1), preferred_element_type=F32)

    def down(stage, c, first, count, landing):
        ahead = AHEAD[first : first + count]
        products = product(stage, c, [others[i] for i in ahead] + [mine[i] for i in ahead])
        for i in range(count):
            psend[stage, first + i, rows_of(c), :] = products[:, BLK * i : BLK * (i + 1)].astype(BF16)
        part = pl.ds(first, count)
        y_copy(psend.at[stage, part, rows_of(c)], precv.at[stage, part, rows_of(c)], stage, c, s_recv.at[c, landing], partner)
        for i in range(count):
            pown[first + i, rows_of(c), :] = products[:, BLK * (count + i) : BLK * (count + i + 1)]

    def down_first(stage, c):
        down(stage, c, 0, 1, 0)

    def down_rest(stage, c):
        down(stage, c, 1, 3, 3)

    def pair_sum(stage, i, rows):
        return pown[i, rows, :] + precv[stage, i, rows, :].astype(F32)

    def sum_a(stage, c):
        await_bytes(precv.at[stage, 0, rows_of(c)], s_recv.at[c, 0])
        s1[stage, rows_of(c), :] = pair_sum(stage, 0, rows_of(c)).astype(BF16)
        for part, device in ((front(c), above), (rear(c), below)):
            y_copy(s1.at[stage, part], r1.at[stage, part], stage, c, s_recv.at[c, 1], device)

    def send_halves(stage, c, parts, with_r1):
        for i, part, device in ((1, parts[0], above), (2, parts[1], below)):
            value = pair_sum(stage, i, part)
            if with_r1:
                value = value + r1[stage, part, :].astype(F32)
            s2[stage, i - 1, part, :] = value.astype(BF16)
            y_copy(s2.at[stage, i - 1, part], r2.at[stage, i - 1, part], stage, c, s_recv.at[c, 2], device)

    def sum_early(stage, c):
        await_bytes(precv.at[stage, pl.ds(1, 3), rows_of(c)], s_recv.at[c, 3])
        send_halves(stage, c, (rear(c), front(c)), False)

    def sum_b(stage, c):
        await_bytes(r1.at[stage, rows_of(c)], s_recv.at[c, 1])
        send_halves(stage, c, (front(c), rear(c)), True)

    def sum_c(stage, c):
        await_bytes(r2.at[stage, pl.ds(0, 2), rows_of(c)], s_recv.at[c, 2])

        rows = rows_of(c)
        branch = pair_sum(stage, 3, rows) + r2[stage, 0, rows, :].astype(F32) + r2[stage, 1, rows, :].astype(F32)
        if stage != 1:
            branch = 0.5 * branch
        value = (xg[stage, t, rows, :].astype(F32) + branch).astype(BF16)
        if stage < 2:
            xg[stage + 1, t, rows, :] = value
            gather_0(stage + 1, c)
        else:
            out[rows, :] = value

    def mid(stage, c):
        if stage == 1:
            mixer(c)
        else:
            ffn(stage, c)

    tasks = dict(
        W=weights, G0=gather_0, G1=gather_1, GH=gather_rest, G2=gather_2, G3=gather_3, N=norm, F=mid,
        DA=down_first, DB=down_rest, SA=sum_a, SE=sum_early, SB=sum_b, SC=sum_c,
    )

    def sent(stage):
        for _ in range(2):
            await_bytes(xg.at[0, pl.ds(0, 7)], y_send.at[stage])

    for step, (name, a, b) in enumerate(ORDER):
        if step == len(ORDER) - 2:
            for g, (first, count) in enumerate(GROUPS):
                await_bytes(w.at[pl.ds(0, 15), pl.ds(first, count)], w_send.at[g])
            sent(0)
            sent(1)
        with jax.named_scope(f"{name}_{a}_{b}"):
            tasks[name](a, b)

    sent(2)


def on_device(
    tokens, first_gain, first_gate, first_up, first_down, mixer_gain, conv_input, outer_gate, inner_gate, conv_taps,
    mixer_out, second_gain, second_gate, second_up, second_down,
):
    shape = tokens.shape
    hbm = pl.BlockSpec(memory_space=pl.ANY)
    dma = pltpu.SemaphoreType.DMA
    result = pl.pallas_call(
        layer_kernel,
        out_shape=pltpu.VMEM((ROWS, BLK), BF16),
        in_specs=[hbm] * 15,
        out_specs=pl.BlockSpec(memory_space=pltpu.VMEM),
        scratch_shapes=[
            pltpu.VMEM((16, SLABS, 128, 128), BF16),
            pltpu.VMEM((3, 8, ROWS, BLK), BF16),
            pltpu.VMEM((ROWS, D), BF16),
            pltpu.VMEM((ROWS, 640), BF16),
            pltpu.VMEM((3, 4, ROWS, BLK), BF16),
            pltpu.VMEM((3, 4, ROWS, BLK), BF16),
            pltpu.VMEM((4, ROWS, BLK), F32),
            pltpu.VMEM((3, ROWS, BLK), BF16),
            pltpu.VMEM((3, ROWS, BLK), BF16),
            pltpu.VMEM((3, 2, ROWS, BLK), BF16),
            pltpu.VMEM((3, 2, ROWS, BLK), BF16),
            pltpu.VMEM((2, 8 + LEN, 128), F32),
            pltpu.VMEM((R, 128), F32),
            pltpu.VMEM((ROWS, 128), BF16),
            pltpu.VMEM((3, 1, D), F32),
            pltpu.VMEM((3, 128), F32),
            dma((2,)),
            dma,
            dma((5,)),
            dma((5, 5)),
            dma((3,)),
            dma((NC, 4)),
            dma((NC, 4)),
            dma((2,)),
        ],
        compiler_params=pltpu.CompilerParams(
            collective_id=0, has_side_effects=True, vmem_limit_bytes=60_000_000
        ),
    )(
        tokens.reshape(ROWS, BLK), first_gain[None], mixer_gain[None], second_gain[None], conv_taps, first_gate, first_up, first_down, conv_input, outer_gate,
        inner_gate, mixer_out, second_gate, second_up, second_down,
    )
    return result.reshape(shape)


def solution(mesh):
    fs, tp = P("fs", "tp"), P("tp", "fs")
    in_specs = (
        P("fs", None, "tp"), P(), fs, fs, tp, P(), fs, fs, fs, P(None, "tp"), tp, P(), fs, fs, tp,
    )
    return jax.shard_map(
        on_device, mesh=mesh, in_specs=in_specs, out_specs=P("fs", None, "tp"), check_vma=False
    )
```

```python
import functools

import jax
import jax.numpy as jnp
from jax import lax
from jax.experimental import pallas as pl
from jax.experimental.pallas import tpu as pltpu
from jax.sharding import PartitionSpec as P

EPS = 1e-05
MESH = pl.DeviceIdType.MESH
F32, BF16 = jnp.float32, jnp.bfloat16

D = 2048
ROWS = 768
LEN = 384
BLK = 256
NC = 4
R = ROWS // NC
HALF = R // 2
SUB = 192
SLABS = 34
GROUPS = ((0, 10), (10, 5), (15, 4), (19, 10), (29, 5))
UNITS = (0, 2, 3, 4, 2, 4)
AHEAD = (2, 1, 3, 0)


ORDER = (
    ("W", 0, 0), ("G0", 0, 2), ("G0", 0, 3), ("G1", 0, 2), ("G0", 0, 0), ("W", 0, 1), ("G1", 0, 0), ("GH", 0, 0),
    ("G1", 0, 3), ("W", 1, 0), ("W", 0, 2), ("G0", 0, 1), ("W", 0, 3), ("G1", 0, 1), ("GH", 0, 1), ("W", 1, 1),
    ("GH", 0, 2), ("G2", 0, 2), ("G3", 0, 2), ("G2", 0, 1), ("GH", 0, 3), ("G2", 0, 0), ("N", 0, 2), ("G2", 0, 3),
    ("G3", 0, 3), ("N", 0, 3), ("G3", 0, 0), ("N", 0, 0), ("W", 1, 2), ("W", 0, 4), ("G3", 0, 1), ("W", 1, 3),
    ("N", 0, 1), ("W", 1, 4), ("W", 2, 0), ("W", 3, 0), ("W", 0, 5), ("F", 0, 3), ("F", 0, 0), ("W", 1, 5),
    ("DA", 0, 0), ("DA", 0, 3), ("DB", 0, 3), ("DB", 0, 0), ("SA", 0, 0), ("SA", 0, 3), ("F", 0, 2), ("DA", 0, 2),
    ("SE", 0, 0), ("DB", 0, 2), ("W", 2, 1), ("SB", 0, 0), ("SE", 0, 3), ("SA", 0, 2), ("F", 0, 1), ("SE", 0, 2),
    ("W", 2, 2), ("SC", 0, 0), ("DA", 0, 1), ("SB", 0, 2), ("SB", 0, 3), ("W", 4, 0), ("G1", 1, 0), ("DB", 0, 1),
    ("W", 2, 3), ("SA", 0, 1), ("W", 2, 4), ("SC", 0, 2), ("W", 3, 1), ("SC", 0, 3), ("GH", 1, 0), ("G2", 1, 0),
    ("G1", 1, 2), ("SE", 0, 1), ("W", 2, 5), ("SB", 0, 1), ("G3", 1, 0), ("N", 1, 0), ("W", 4, 1), ("GH", 1, 2),
    ("F", 1, 0), ("DA", 1, 0), ("DB", 1, 0), ("G1", 1, 3), ("G2", 1, 2), ("SA", 1, 0), ("SC", 0, 1), ("GH", 1, 3),
    ("G2", 1, 3), ("G3", 1, 2), ("N", 1, 2), ("F", 1, 2), ("SE", 1, 0), ("DA", 1, 2), ("SB", 1, 0), ("DB", 1, 2),
    ("W", 3, 2), ("G3", 1, 3), ("N", 1, 3), ("G1", 1, 1), ("F", 1, 3), ("DA", 1, 3), ("W", 3, 3), ("SA", 1, 2),
    ("SE", 1, 2), ("DB", 1, 3), ("GH", 1, 1), ("SA", 1, 3), ("G2", 1, 1), ("SC", 1, 0), ("SE", 1, 3), ("W", 4, 2),
    ("G3", 1, 1), ("N", 1, 1), ("F", 1, 1), ("SB", 1, 3), ("DA", 1, 1), ("SB", 1, 2), ("G1", 2, 0), ("GH", 2, 0),
    ("DB", 1, 1), ("W", 3, 4), ("W", 4, 3), ("SA", 1, 1), ("SC", 1, 3), ("G2", 2, 0), ("SE", 1, 1), ("SB", 1, 1),
    ("W", 4, 4), ("G1", 2, 3), ("GH", 2, 3), ("G3", 2, 0), ("SC", 1, 2), ("N", 2, 0), ("W", 3, 5), ("F", 2, 0),
    ("SC", 1, 1), ("G2", 2, 3), ("G1", 2, 2), ("W", 4, 5), ("DA", 2, 0), ("DB", 2, 0), ("GH", 2, 2), ("G3", 2, 3),
    ("N", 2, 3), ("G1", 2, 1), ("F", 2, 3), ("DA", 2, 3), ("G2", 2, 2), ("GH", 2, 1), ("SA", 2, 0), ("SE", 2, 0),
    ("DB", 2, 3), ("G2", 2, 1), ("SA", 2, 3), ("G3", 2, 2), ("N", 2, 2), ("F", 2, 2), ("DA", 2, 2), ("SB", 2, 0),
    ("SE", 2, 3), ("G3", 2, 1), ("N", 2, 1), ("F", 2, 1), ("DA", 2, 1), ("SA", 2, 2), ("DB", 2, 2), ("SB", 2, 3),
    ("DB", 2, 1), ("SC", 2, 0), ("SA", 2, 1), ("SE", 2, 2), ("SB", 2, 2), ("SE", 2, 1), ("SC", 2, 3), ("SB", 2, 1),
    ("SC", 2, 2), ("SC", 2, 1),
)


def layer_kernel(
    tokens, gain_1, gain_2, gain_3, taps_in, fgate, fup, fdown, conv_in, outer_gate, inner_gate, mix_out, sgate, sup, sdown,
    out,
    w, xg, normed, hidden, psend, precv, pown, s1, r1, s2, r2, gi, outer_s, mixed, gains, taps,
    w_load, x_load, w_send, w_recv, y_send, g_recv, s_recv, k_load,
):
    f, t = lax.axis_index("fs"), lax.axis_index("tp")
    z, x = lax.div(f, 4), lax.rem(f, 4)
    y, core = lax.div(t, 2), lax.rem(t, 2)
    other = 1 - core
    zs = [4 * lax.rem(z + i, 4) for i in range(4)]
    xs = [lax.rem(x + i, 4) for i in range(4)]
    ys = [2 * lax.rem(y + i, 4) for i in range(4)]
    slots = [[zs[i] + xs[j] for j in range(4)] for i in range(4)]
    mine, others = [a + core for a in ys], [a + other for a in ys]

    def slot(h, a, b):
        return slots[b][a] if h == 0 else slots[a][b]

    def w_device(h, phase, d):
        return (slot(h, d, 0) if phase == 1 else slot(h, 0, d), t)

    above, below, partner = (f, mine[1]), (f, mine[3]), (f, others[0])

    def load_tokens():
        return pltpu.make_async_copy(tokens, xg.at[0, t], x_load)

    def loads(g):
        sources = []
        if g in (0, 3):
            for s in range(5):
                for a in (fgate, fup) if g == 0 else (sgate, sup):
                    sources.append(a.at[:, pl.ds(128 * s, 128)])
        elif g in (1, 4):
            a = fdown if g == 1 else sdown
            sources = [a.at[pl.ds(128 * s, 128), :] for s in range(5)]
        else:
            sources = [conv_in, outer_gate, inner_gate, mix_out]
        first = GROUPS[g][0]
        return [pltpu.make_async_copy(a, w.at[f, first + i], w_load.at[min(g, 1)]) for i, a in enumerate(sources)]

    def await_bytes(ref, sem):
        pltpu.make_async_copy(ref, ref, sem).wait()

    def load_vectors():
        copies = [pltpu.make_async_copy(a, gains.at[i], k_load.at[0]) for i, a in enumerate((gain_1, gain_2, gain_3))]
        return copies + [pltpu.make_async_copy(taps_in, taps, k_load.at[1])]

    load_tokens().start()
    for g in range(5):
        for copy in loads(g):
            copy.start()
    for copy in load_vectors():
        copy.start()

    barrier = pltpu.get_barrier_semaphore()
    peers = [w_device(h, 1, d) for h in (0, 1) for d in (1, 3)] + [above, below, partner]
    for peer in peers:
        pl.semaphore_signal(barrier, inc=1, device_id=peer, device_id_type=MESH)

    gi[:, pl.ds(0, 8), :] = jnp.zeros((2, 8, 128), F32)

    load_tokens().wait()
    await_bytes(gains, k_load.at[0])
    await_bytes(taps, k_load.at[1])
    pl.semaphore_wait(barrier, len(peers))

    def w_copy(g, h, a, b, phase, d, quarter, landing):
        first, count = GROUPS[g]
        if quarter:
            rows = pl.ds(64 * h + (0 if (d == 1) == (quarter == 1) else 32), 32)
        else:
            rows = pl.ds(64 * h, 64)
        part = w.at[slot(h, a, b), pl.ds(first, count), rows]
        pltpu.make_async_remote_copy(
            src_ref=part, dst_ref=part, send_sem=w_send.at[g], recv_sem=w_recv.at[g, landing - 1],
            device_id=w_device(h, phase, d), device_id_type=MESH,
        ).start()

    def w_wait(g, landing):
        first, count = GROUPS[g]
        await_bytes(w.at[pl.ds(0, UNITS[landing]), pl.ds(first, count)], w_recv.at[g, landing - 1])

    both = [(h, d) for h in (0, 1) for d in (1, 3)]

    def weights(g, rnd):
        first, count = GROUPS[g]
        if rnd == 0:
            if g < 2:
                loaded = pl.ds(0, 10) if g == 0 else pl.ds(10, SLABS - 10)
                await_bytes(w.at[f, loaded], w_load.at[g])
            for h, d in both:
                w_copy(g, h, 0, 0, 1, d, 0, 1)
            for h, d in both:
                w_copy(g, h, 0, 0, 2, d, 0, 2)
        elif rnd == 5:
            w_wait(g, 5)
        else:
            w_wait(g, rnd)
            for h, d in both:
                back = 4 - d
                if rnd == 1:
                    w_copy(g, h, back, 0, 1, d, 1, 2)
                elif rnd == 2:
                    w_copy(g, h, 0, back, 2, d, 1, 4)
                    w_copy(g, h, 2, 0, 2, d, 1, 4)
                elif rnd == 3:
                    w_copy(g, h, 1, back, 2, d, 1, 5)
                    w_copy(g, h, 3, back, 2, d, 1, 5)
                else:
                    w_copy(g, h, 2, back, 2, d, 1, 5)
            for h, d in both:
                if rnd == 1:
                    w_copy(g, h, 1, 0, 2, d, 0, 3)
                    w_copy(g, h, 3, 0, 2, d, 0, 3)
                elif rnd == 2:
                    w_copy(g, h, 2, 0, 2, d, 2, 5)

    def y_copy(src, dst, stage, c, recv, device):
        pltpu.make_async_remote_copy(
            src_ref=src, dst_ref=dst, send_sem=y_send.at[stage], recv_sem=recv,
            device_id=device, device_id_type=MESH,
        ).start()

    def rows_of(c):
        return pl.ds(c * R, R)

    def front(c):
        return pl.ds(c * R, HALF)

    def rear(c):
        return pl.ds(c * R + HALF, HALF)

    def gather_0(stage, c):
        ref = xg.at[stage, t, rows_of(c)]
        for landing, parts in ((0, (front(c), rear(c))), (3, (rear(c), front(c)))):
            for part, device in zip(parts, (above, below)):
                half = xg.at[stage, t, part]
                y_copy(half, half, stage, c, g_recv.at[c, landing], device)
        y_copy(ref, ref, stage, c, g_recv.at[c, 2], partner)

    def gather_1(stage, c):
        await_bytes(xg.at[stage, 0, rows_of(c)], g_recv.at[c, 0])
        for block, part, device in ((mine[3], front(c), above), (mine[1], rear(c), below)):
            ref = xg.at[stage, block, part]
            y_copy(ref, ref, stage, c, g_recv.at[c, 1], device)

    def gather_rest(stage, c):
        await_bytes(xg.at[stage, 0, rows_of(c)], g_recv.at[c, 3])
        for block in (mine[3], mine[1]):
            ref = xg.at[stage, block, rows_of(c)]
            y_copy(ref, ref, stage, c, g_recv.at[c, 2], partner)

    def gather_2(stage, c):
        await_bytes(xg.at[stage, 0, rows_of(c)], g_recv.at[c, 1])
        ref = xg.at[stage, mine[2], rows_of(c)]
        y_copy(ref, ref, stage, c, g_recv.at[c, 2], partner)

    def gather_3(stage, c):
        await_bytes(xg.at[stage, pl.ds(0, 4), rows_of(c)], g_recv.at[c, 2])

    def norm(stage, c):
        @pl.loop(0, R // SUB)
        def _(i):
            rows = pl.ds(pl.multiple_of(c * R + i * SUB, SUB), SUB)
            total = jnp.zeros((SUB, BLK), F32)
            for b in range(8):
                v = xg[stage, b, rows, :].astype(F32)
                total = total + v * v
            mean = jnp.sum(total, axis=1, keepdims=True) * (1.0 / D)
            scale = lax.rsqrt(mean + EPS)
            for b in range(8):
                v = xg[stage, b, rows, :].astype(F32)
                cols = pl.ds(b * BLK, BLK)
                normed[rows, cols] = (v * scale * gains[stage, :, cols]).astype(BF16)

    def columns(first):
        return w[:, first].reshape(D, 128)

    def ffn(stage, c):
        first = 0 if stage == 0 else 19

        all_columns = jnp.concatenate([columns(first + 2 * s + i) for i in (0, 1) for s in range(5)], axis=1)
        products = jnp.dot(normed[rows_of(c), :], all_columns, preferred_element_type=F32)
        gate, upward = products[:, :640], products[:, 640:]
        hidden[rows_of(c), :] = (gate / (1.0 + jnp.exp(-gate)) * upward).astype(BF16)

    def mixer(c):
        three = jnp.concatenate([columns(15), columns(16), columns(17)], axis=1)
        products = jnp.dot(normed[rows_of(c), :], three, preferred_element_type=F32)
        seq, at = c * R // LEN, c * R % LEN
        gi[seq, pl.ds(8 + at, R), :] = products[:, 256:] * products[:, :128]
        outer_s[...] = products[:, 128:256]
        convolved = taps[0:1, :] * gi[seq, pl.ds(6 + at, R), :]
        convolved = convolved + taps[1:2, :] * gi[seq, pl.ds(7 + at, R), :]
        convolved = convolved + taps[2:3, :] * gi[seq, pl.ds(8 + at, R), :]
        mixed[rows_of(c), :] = (outer_s[...] * convolved).astype(BF16)

    def product(stage, c, blocks):
        if stage == 1:
            rows, columns = mixed[rows_of(c), :], [w[2 * b + i, 18] for b in blocks for i in (0, 1)]
        else:
            slabs = pl.ds(10 if stage == 0 else 29, 5)
            rows, columns = hidden[rows_of(c), :], [w[2 * b + i, slabs].reshape(640, 128) for b in blocks for i in (0, 1)]
        return jnp.dot(rows, jnp.concatenate(columns, axis=1), preferred_element_type=F32)

    def down(stage, c, first, count, landing):
        ahead = AHEAD[first : first + count]
        products = product(stage, c, [others[i] for i in ahead] + [mine[i] for i in ahead])
        for i in range(count):
            psend[stage, first + i, rows_of(c), :] = products[:, BLK * i : BLK * (i + 1)].astype(BF16)
        part = pl.ds(first, count)
        y_copy(psend.at[stage, part, rows_of(c)], precv.at[stage, part, rows_of(c)], stage, c, s_recv.at[c, landing], partner)
        for i in range(count):
            pown[first + i, rows_of(c), :] = products[:, BLK * (count + i) : BLK * (count + i + 1)]

    def down_first(stage, c):
        down(stage, c, 0, 1, 0)

    def down_rest(stage, c):
        down(stage, c, 1, 3, 3)

    def pair_sum(stage, i, rows):
        return pown[i, rows, :] + precv[stage, i, rows, :].astype(F32)

    def sum_a(stage, c):
        await_bytes(precv.at[stage, 0, rows_of(c)], s_recv.at[c, 0])
        s1[stage, rows_of(c), :] = pair_sum(stage, 0, rows_of(c)).astype(BF16)
        for part, device in ((front(c), above), (rear(c), below)):
            y_copy(s1.at[stage, part], r1.at[stage, part], stage, c, s_recv.at[c, 1], device)

    def send_halves(stage, c, parts, with_r1):
        for i, part, device in ((1, parts[0], above), (2, parts[1], below)):
            value = pair_sum(stage, i, part)
            if with_r1:
                value = value + r1[stage, part, :].astype(F32)
            s2[stage, i - 1, part, :] = value.astype(BF16)
            y_copy(s2.at[stage, i - 1, part], r2.at[stage, i - 1, part], stage, c, s_recv.at[c, 2], device)

    def sum_early(stage, c):
        await_bytes(precv.at[stage, pl.ds(1, 3), rows_of(c)], s_recv.at[c, 3])
        send_halves(stage, c, (rear(c), front(c)), False)

    def sum_b(stage, c):
        await_bytes(r1.at[stage, rows_of(c)], s_recv.at[c, 1])
        send_halves(stage, c, (front(c), rear(c)), True)

    def sum_c(stage, c):
        await_bytes(r2.at[stage, pl.ds(0, 2), rows_of(c)], s_recv.at[c, 2])

        rows = rows_of(c)
        branch = pair_sum(stage, 3, rows) + r2[stage, 0, rows, :].astype(F32) + r2[stage, 1, rows, :].astype(F32)
        if stage != 1:
            branch = 0.5 * branch
        value = (xg[stage, t, rows, :].astype(F32) + branch).astype(BF16)
        if stage < 2:
            xg[stage + 1, t, rows, :] = value
            gather_0(stage + 1, c)
        else:
            out[rows, :] = value

    def mid(stage, c):
        if stage == 1:
            mixer(c)
        else:
            ffn(stage, c)

    tasks = dict(
        W=weights, G0=gather_0, G1=gather_1, GH=gather_rest, G2=gather_2, G3=gather_3, N=norm, F=mid,
        DA=down_first, DB=down_rest, SA=sum_a, SE=sum_early, SB=sum_b, SC=sum_c,
    )

    def sent(stage):
        for _ in range(2):
            await_bytes(xg.at[0, pl.ds(0, 7)], y_send.at[stage])

    for step, (name, a, b) in enumerate(ORDER):
        if step == len(ORDER) - 2:
            for g, (first, count) in enumerate(GROUPS):
                await_bytes(w.at[pl.ds(0, 15), pl.ds(first, count)], w_send.at[g])
            sent(0)
            sent(1)
        with jax.named_scope(f"{name}_{a}_{b}"):
            tasks[name](a, b)

    sent(2)


def on_device(
    tokens, first_gain, first_gate, first_up, first_down, mixer_gain, conv_input, outer_gate, inner_gate, conv_taps,
    mixer_out, second_gain, second_gate, second_up, second_down,
):
    shape = tokens.shape
    hbm = pl.BlockSpec(memory_space=pl.ANY)
    dma = pltpu.SemaphoreType.DMA
    result = pl.pallas_call(
        layer_kernel,
        out_shape=pltpu.VMEM((ROWS, BLK), BF16),
        in_specs=[hbm] * 15,
        out_specs=pl.BlockSpec(memory_space=pltpu.VMEM),
        scratch_shapes=[
            pltpu.VMEM((16, SLABS, 128, 128), BF16),
            pltpu.VMEM((3, 8, ROWS, BLK), BF16),
            pltpu.VMEM((ROWS, D), BF16),
            pltpu.VMEM((ROWS, 640), BF16),
            pltpu.VMEM((3, 4, ROWS, BLK), BF16),
            pltpu.VMEM((3, 4, ROWS, BLK), BF16),
            pltpu.VMEM((4, ROWS, BLK), F32),
            pltpu.VMEM((3, ROWS, BLK), BF16),
            pltpu.VMEM((3, ROWS, BLK), BF16),
            pltpu.VMEM((3, 2, ROWS, BLK), BF16),
            pltpu.VMEM((3, 2, ROWS, BLK), BF16),
            pltpu.VMEM((2, 8 + LEN, 128), F32),
            pltpu.VMEM((R, 128), F32),
            pltpu.VMEM((ROWS, 128), BF16),
            pltpu.VMEM((3, 1, D), F32),
            pltpu.VMEM((3, 128), F32),
            dma((2,)),
            dma,
            dma((5,)),
            dma((5, 5)),
            dma((3,)),
            dma((NC, 4)),
            dma((NC, 4)),
            dma((2,)),
        ],
        compiler_params=pltpu.CompilerParams(
            collective_id=0, has_side_effects=True, vmem_limit_bytes=60_000_000
        ),
    )(
        tokens.reshape(ROWS, BLK), first_gain[None], mixer_gain[None], second_gain[None], conv_taps, first_gate, first_up, first_down, conv_input, outer_gate,
        inner_gate, mixer_out, second_gate, second_up, second_down,
    )
    return result.reshape(shape)


def solution(mesh):
    fs, tp = P("fs", "tp"), P("tp", "fs")
    in_specs = (
        P("fs", None, "tp"), P(), fs, fs, tp, P(), fs, fs, fs, P(None, "tp"), tp, P(), fs, fs, tp,
    )
    return jax.shard_map(
        on_device, mesh=mesh, in_specs=in_specs, out_specs=P("fs", None, "tp"), check_vma=False
    )
```
